32 devices in a mesh: sp: 16 (over z, y, x), dp: 2 (over core).
Axes of the slice: x: 2, y: 2, z: 4, core: 2. Of those that a mesh axis runs over, the one named last changes fastest.
Arguments:
- queries: bfloat16 [2, 2048, 3072], P('dp', 'sp'), may hold values from -20 to 20
- kv_latent: bfloat16 [2, 2048, 256], P('dp', 'sp'), may hold values from -60 to 60
- rope_key: bfloat16 [2, 2048, 32], P('dp', 'sp'), may hold values from -20 to 20
- latent_norm_gain: float32 [256], replicated, may hold values from 0.1 to 1.9
- key_up_weight: bfloat16 [256, 2048], replicated, may hold values from -0.375 to 0.375
- value_up_weight: bfloat16 [256, 2048], replicated, may hold values from -0.375 to 0.375
- out_proj: bfloat16 [2048, 2048], replicated, may hold values from -0.125 to 0.125
- residual: bfloat16 [2, 2048, 2048], P('dp', 'sp'), may hold values from -0.59765625 to 0.59765625
- ffn_gain: float32 [2048], replicated, may hold values from 0.1 to 1.9
- routes: int32 [2, 2048, 2], P('dp', 'sp'), may hold values from 0 to 31, all different within a row; in each aligned block of 128 rows (0 to 127, 128 to 255, ..., all dimensions but the last counted through in order) at most 16 rows name the same one
- route_weights: float32 [2, 2048, 2], P('dp', 'sp'), may hold values from 0.1 to 1
- expert_gate: bfloat16 [32, 2048, 1024], P(('sp', 'dp')), may hold values from -1.3258252 to 1.3258252
- expert_up: bfloat16 [32, 2048, 1024], P(('sp', 'dp')), may hold values from -1.3258252 to 1.3258252
- expert_down: bfloat16 [32, 1024, 2048], P(('sp', 'dp')), may hold values from -0.1875 to 0.1875
Outputs:
- normed_rows: bfloat16 [2, 2048, 2048], P('dp', 'sp')
- layer_out: bfloat16 [2, 2048, 2048], P('dp', 'sp')
The draws below stay inside these ranges and needn't reach their ends.
Inputs may be any that keep to these rules, and one draw needn't show every extreme that they name: `routes`: each token names 2 different experts. Among the tokens of one device no expert is named more than 16 times, and in some devices' tokens an expert is named exactly 16 times.
All inputs are finite; a program needn't handle non-finite values.
Results may differ from the reference program's by a relative error of at most 0.012.
The reference program's roundings to bfloat16 on the way count: a program that leaves them out, or rounds other values in their place, can miss the bound.
Values may be sent and summed in bfloat16 or wider, within the bound.
A program may use at most 128 MiB of HBM per device.

```python
import math
import jax
import jax.numpy as jnp
import numpy as np
from jax import lax

D = 2048
HEAD_COUNT = 32
PLAIN_HEAD_SIZE = 64
ROTARY_SIZE = 32
VALUE_HEAD_SIZE = 64
LATENT_WIDTH = 256
FF = 1024
TOPK = 2
GRID_W = 64
TOK_DEV = 128
SEQUENCE_LENGTH = 2048
SEQUENCE_COUNT = 2
EXPERTS = 32
CAP = 16


def draw_rope_key(key, part):
    child_random_key = jax.random.fold_in(key, 3)
    return jnp.clip(jax.random.normal(child_random_key, (SEQUENCE_COUNT, SEQUENCE_LENGTH, ROTARY_SIZE), jnp.float32), -6.0, 6.0).astype(jnp.bfloat16)


def draw_queries(key, part):
    child_random_key = jax.random.fold_in(key, 5)
    shape = (SEQUENCE_COUNT, SEQUENCE_LENGTH, HEAD_COUNT, PLAIN_HEAD_SIZE + ROTARY_SIZE)
    starting_random = jnp.clip(2.0 * jax.random.normal(child_random_key, shape, jnp.float32), -12.0, 12.0)
    return starting_random.reshape(SEQUENCE_COUNT, SEQUENCE_LENGTH, HEAD_COUNT * (PLAIN_HEAD_SIZE + ROTARY_SIZE)).astype(jnp.bfloat16)


def draw_kv_latent(key, part):
    child_random_key = jax.random.fold_in(key, 9)
    starting_random = jnp.clip(jax.random.normal(child_random_key, (SEQUENCE_COUNT, SEQUENCE_LENGTH, LATENT_WIDTH), jnp.float32), -6.0, 6.0)
    return starting_random.astype(jnp.bfloat16)


def expert_matrix(key, salt):
    child_random_key = jax.random.fold_in(key, salt)
    starting_random = jnp.clip(jax.random.normal(child_random_key, (EXPERTS, D, FF), jnp.float32), -6.0, 6.0) * D ** (-0.5)
    return starting_random.astype(jnp.bfloat16)


def draw_expert_gate(key, part):
    return expert_matrix(key, 21)


def draw_expert_up(key, part):
    return expert_matrix(key, 23)


def block_levels(key, dims, pieces, low, largest):
    factor_of = 1.0
    for axis_at, shards_of in pieces:
        heights = jax.random.uniform(jax.random.fold_in(jax.random.fold_in(key, 6), axis_at), (shards_of,), jnp.float32, low / len(pieces), largest / len(pieces))
        factor_of = factor_of * jnp.repeat(jnp.exp(heights), dims[axis_at] // shards_of).reshape((-1,) + (1,) * (len(dims) - 1 - axis_at))
    return factor_of


def deal_out(rng, own, number, rows, count, top, reach, lean):
    ranking = jax.random.permutation(rng, count)
    packed, usual = shares(count, rows * top, reach, lean, True), shares(count, rows * top, reach, lean, False)
    places = jnp.arange(count)

    def named(lengths, offset_by):
        used = int((lengths > 0).sum())
        fixed = max(1, used // 4)
        moved = fixed + (places - fixed + offset_by * (used - fixed)) % max(1, count - fixed)
        return jnp.zeros((count,), jnp.int32).at[ranking[jnp.where(places < fixed, places, moved)]].set(jnp.asarray(lengths, jnp.int32))

    lengths = jnp.where(number % 4 == 0, named(packed, number // 4), named(usual, number - number // 4 - 1))
    mixed = jax.random.permutation(jax.random.fold_in(own, 3), count)
    donor, taker = mixed[0:count // 2 * 2:2], mixed[1:count // 2 * 2:2]
    slack = jnp.minimum(lengths[donor] - 1, reach - lengths[taker]) // 2
    slack = jnp.where((donor == ranking[0]) | (taker == ranking[0]) | (lengths[taker] == 0), 0, jnp.maximum(slack, 0))
    moved = jax.random.randint(jax.random.fold_in(own, 4), (count // 2,), 0, 1 << 20) % (slack + 1)
    lengths = lengths.at[donor].add(-moved).at[taker].add(moved)
    labels = jnp.searchsorted(jnp.cumsum(lengths), jnp.arange(rows * top), side="right").astype(jnp.int32)
    grid = labels.reshape(top, rows).T
    grid = grid[jax.random.permutation(jax.random.fold_in(own, 1), rows)]
    offset_by = jax.random.randint(jax.random.fold_in(own, 2), (rows, 1), 0, top)
    return jnp.take_along_axis(grid, (jnp.arange(top)[None, :] + offset_by) % top, axis=1)


def shares(count, total, bound, slope, full):
    loads = [(1 << 20) // math.isqrt(grade ** slope) + 1 for grade in range(1, count + 1)]
    largest = bound if full else min(bound, max(-(-total // count), total * loads[0] // sum(loads)))
    least = 1 if total - largest >= count - 1 else 0
    given, rest = [largest] + [least] * (count - 1), total - largest - least * (count - 1)
    while rest > 0:
        candidates = [i for i in range(1, count) if given[i] < largest] or [i for i in range(1, count) if given[i] < bound]
        whole, budget = sum([loads[i] for i in candidates]), rest
        for i in candidates:
            extra = min(bound - given[i], max(1, budget * loads[i] // whole), rest)
            given[i] = given[i] + extra
            rest = rest - extra
    return np.array(given)


def bell_draw(rng, dims, width, reach, shards=(), kind=jnp.bfloat16):
    values = jax.random.normal(rng, dims, jnp.float32) * width
    if len(shards) > 0:
        values = block_levels(rng, dims, shards, -0.22, 0.18) * values
    return jnp.clip(values, min=-reach, max=reach).astype(kind)


def setup_inputs(seed: int = 0) -> dict:
    seeds = jax.random.split(jax.random.key(seed), 15)
    queries = draw_queries(jax.random.fold_in(seeds[14], 71), 0)
    kv_latent = draw_kv_latent(jax.random.fold_in(seeds[14], 71), 0)
    rope_key = draw_rope_key(jax.random.fold_in(seeds[14], 71), 0)
    latent_norm_gain = jnp.clip(1.0 + 0.18 * jax.random.normal(seeds[3], (LATENT_WIDTH,), jnp.float32), 0.1, 1.9)
    key_up_weight = bell_draw(seeds[4], (LATENT_WIDTH, HEAD_COUNT * PLAIN_HEAD_SIZE), LATENT_WIDTH ** -0.5, 0.375)
    value_up_weight = bell_draw(seeds[5], (LATENT_WIDTH, HEAD_COUNT * VALUE_HEAD_SIZE), LATENT_WIDTH ** -0.5, 0.375)
    out_proj = bell_draw(seeds[6], (HEAD_COUNT * VALUE_HEAD_SIZE, D), (HEAD_COUNT * VALUE_HEAD_SIZE) ** -0.5, 0.125)
    residual = bell_draw(seeds[7], (SEQUENCE_COUNT, SEQUENCE_LENGTH, D), 0.1, 0.59765625, ((0, 2), (1, 16)))
    ffn_gain = jnp.clip(1.0 + 0.18 * jax.random.normal(seeds[8], (D,), jnp.float32), 0.1, 1.9)
    routes_keys = jax.random.split(jax.random.fold_in(seeds[9], 1), SEQUENCE_COUNT * SEQUENCE_LENGTH // TOK_DEV)
    routes_turns = jax.random.permutation(jax.random.fold_in(seeds[9], 3), SEQUENCE_COUNT * SEQUENCE_LENGTH // TOK_DEV)
    routes = jax.vmap(lambda own, number: deal_out(jax.random.fold_in(seeds[9], 2), own, number, TOK_DEV, EXPERTS, TOPK, CAP, 2))(routes_keys, routes_turns).reshape((SEQUENCE_COUNT, SEQUENCE_LENGTH, TOPK))
    route_weights = jnp.clip(jnp.exp(math.log(1.0) - 2.3025851 * jax.random.uniform(seeds[10], (SEQUENCE_COUNT, SEQUENCE_LENGTH, TOPK), jnp.float32) ** block_levels(seeds[10], (SEQUENCE_COUNT, SEQUENCE_LENGTH, TOPK), ((0, 2), (1, 16)), -0.2, 0.2)), 0.1, 1.0)
    expert_gate = draw_expert_gate(jax.random.fold_in(seeds[14], 71), 0)
    expert_up = draw_expert_up(jax.random.fold_in(seeds[14], 71), 0)
    expert_down = bell_draw(seeds[13], (EXPERTS, FF, D), FF ** -0.5, 0.1875, ((0, 32),))
    return {"queries": queries, "kv_latent": kv_latent, "rope_key": rope_key, "latent_norm_gain": latent_norm_gain, "key_up_weight": key_up_weight, "value_up_weight": value_up_weight, "out_proj": out_proj, "residual": residual, "ffn_gain": ffn_gain, "routes": routes, "route_weights": route_weights, "expert_gate": expert_gate, "expert_up": expert_up, "expert_down": expert_down}


eps_norm = 1e-06
rope_base = 10000.0
clamp_limit = 7.0
glu_alpha = 1.702

def rope_tables(positions):
    grid_row = (positions // GRID_W).astype(jnp.float32)
    grid_col = (positions % GRID_W).astype(jnp.float32)
    quarter = ROTARY_SIZE // 4
    frequency = rope_base ** (-(2.0 * jnp.arange(quarter, dtype=jnp.float32)) / (ROTARY_SIZE // 2))
    angles = jnp.concatenate([grid_row[:, None] * frequency[None, :], grid_col[:, None] * frequency[None, :]], axis=1)
    return (jnp.cos(angles), jnp.sin(angles))

def rotate(entries, cosine_table, sine_table):
    pair_view = entries.reshape(entries.shape[:-1] + (entries.shape[-1] // 2, 2))
    first_half = pair_view[..., 0]
    second_half = pair_view[..., 1]
    turned = jnp.stack([first_half * cosine_table - second_half * sine_table, first_half * sine_table + second_half * cosine_table], axis=-1)
    return turned.reshape(entries.shape)

def rms_scale(entries, gain_vec):
    floats = entries.astype(jnp.float32)
    return floats * lax.rsqrt(lax.optimization_barrier(jnp.mean(floats * floats, axis=-1, keepdims=True)) + eps_norm) * gain_vec.astype(jnp.float32)

def clamped_unit(gate_pre, up_pre):
    gate_cut = jnp.minimum(gate_pre, clamp_limit)
    up_cut = jnp.clip(up_pre, -clamp_limit, clamp_limit)
    return gate_cut * jax.nn.sigmoid(glu_alpha * gate_cut) * (up_cut + 1.0)

def expert_rows(rows, gate_w, up_w, down_w):
    gate_pre = jnp.dot(rows, gate_w, preferred_element_type=jnp.float32)
    up_pre = jnp.dot(rows, up_w, preferred_element_type=jnp.float32)
    hidden = clamped_unit(gate_pre, up_pre).astype(jnp.bfloat16)
    return jnp.dot(hidden, down_w, preferred_element_type=jnp.float32).astype(jnp.bfloat16)

def attend_sequence(query_rows, key_row_list, value_per_head):
    token_length = query_rows.shape[0]
    block_row_count = min(512, token_length)
    blocks = query_rows.reshape(token_length // block_row_count, block_row_count, query_rows.shape[1], query_rows.shape[2])
    key_single_float = key_row_list.astype(jnp.float32)
    latent_single_float = key_single_float[:, :LATENT_WIDTH]
    value_float = value_per_head.astype(jnp.float32)

    def one_block(query_block):
        scores = jnp.einsum('qhd,kd->hqk', query_block.astype(jnp.float32), key_single_float)
        highest = lax.optimization_barrier(jnp.max(scores, axis=-1, keepdims=True))
        weights = jnp.exp(scores - highest)
        weights_brain_float = (weights / lax.optimization_barrier(jnp.sum(weights, axis=-1, keepdims=True))).astype(jnp.bfloat16)
        context = jnp.einsum('nef,fg->eng', weights_brain_float.astype(jnp.float32), latent_single_float).astype(jnp.bfloat16)
        return jnp.einsum('qhc,chv->qhv', context.astype(jnp.float32), value_float).astype(jnp.bfloat16)
    result = lax.map(one_block, blocks)
    return result.reshape(token_length, query_rows.shape[1] * VALUE_HEAD_SIZE)

def route_sum(normed, flat_expert, flat_weight, expert_gate, expert_up, expert_down):
    count_rows = normed.shape[0]
    assign_count = flat_expert.shape[0]
    block_row_count = 128
    sort_order = jnp.argsort(flat_expert, stable=True).astype(jnp.int32)
    sorted_expert = flat_expert[sort_order]
    counts = jnp.bincount(flat_expert, length=EXPERTS).astype(jnp.int32)
    starts = (jnp.cumsum(counts) - counts).astype(jnp.int32)
    padded = ((counts + block_row_count - 1) // block_row_count * block_row_count).astype(jnp.int32)
    pad_ends = jnp.cumsum(padded).astype(jnp.int32)
    pad_starts = (pad_ends - padded).astype(jnp.int32)
    slot_index = (pad_starts[sorted_expert] + jnp.arange(assign_count, dtype=jnp.int32) - starts[sorted_expert]).astype(jnp.int32)
    block_count = (assign_count + EXPERTS * (block_row_count - 1)) // block_row_count + 1
    slot_total = block_count * block_row_count
    slot_token = jnp.full((slot_total,), count_rows, jnp.int32).at[slot_index].set((sort_order // TOPK).astype(jnp.int32))
    slot_weight = jnp.zeros((slot_total,), jnp.float32).at[slot_index].set(flat_weight[sort_order].astype(jnp.float32))
    block_starts = jnp.arange(block_count, dtype=jnp.int32) * block_row_count
    block_expert = jnp.minimum(jnp.searchsorted(pad_ends, block_starts, side='right'), EXPERTS - 1).astype(jnp.int32)
    padded_rows = jnp.concatenate([normed, jnp.zeros((1, normed.shape[1]), normed.dtype)], axis=0)

    def one_block(pair):
        tokens, expert = pair
        rows = padded_rows[tokens]
        return expert_rows(rows, expert_gate[expert], expert_up[expert], expert_down[expert]).astype(jnp.float32)
    outputs = lax.map(one_block, (slot_token.reshape(block_count, block_row_count), block_expert))
    outputs = outputs.reshape(slot_total, normed.shape[1]) * slot_weight[:, None]
    return jax.ops.segment_sum(outputs, slot_token, num_segments=count_rows + 1)[:count_rows]

def reference(queries, kv_latent, rope_key, latent_norm_gain, key_up_weight, value_up_weight, out_proj, residual, ffn_gain, routes, route_weights, expert_gate, expert_up, expert_down):
    positions = jnp.arange(SEQUENCE_LENGTH, dtype=jnp.int32)
    cosine_table, sine_table = rope_tables(positions)
    score_scale = (PLAIN_HEAD_SIZE + ROTARY_SIZE) ** (-0.5)
    query_float = queries.astype(jnp.float32).reshape(SEQUENCE_COUNT, SEQUENCE_LENGTH, HEAD_COUNT, PLAIN_HEAD_SIZE + ROTARY_SIZE)
    query_turned = rotate(query_float[..., PLAIN_HEAD_SIZE:], cosine_table[None, :, None, :], sine_table[None, :, None, :])
    q_ready = (jnp.concatenate([query_float[..., :PLAIN_HEAD_SIZE], query_turned], axis=-1) * score_scale).astype(jnp.bfloat16)
    key_turned = rotate(rope_key.astype(jnp.float32), cosine_table[None], sine_table[None]).astype(jnp.bfloat16)
    latent = rms_scale(kv_latent, latent_norm_gain).astype(jnp.bfloat16)
    key_per_head = key_up_weight.astype(jnp.float32).reshape(LATENT_WIDTH, HEAD_COUNT, PLAIN_HEAD_SIZE)
    value_per_head = value_up_weight.reshape(LATENT_WIDTH, HEAD_COUNT, VALUE_HEAD_SIZE)
    key_row_list = jnp.concatenate([latent, key_turned], axis=-1)

    def per_sequence(pair):
        q_seq, key_seq = pair
        q_latent = jnp.einsum('qhn,chn->qhc', q_seq[..., :PLAIN_HEAD_SIZE].astype(jnp.float32), key_per_head).astype(jnp.bfloat16)
        query_complete = jnp.concatenate([q_latent, q_seq[..., PLAIN_HEAD_SIZE:]], axis=-1)
        return attend_sequence(query_complete, key_seq, value_per_head)
    heads_out = lax.map(per_sequence, (q_ready, key_row_list))
    mixed = residual.reshape(SEQUENCE_COUNT * SEQUENCE_LENGTH, D).astype(jnp.float32) + jnp.dot(heads_out.reshape(SEQUENCE_COUNT * SEQUENCE_LENGTH, HEAD_COUNT * VALUE_HEAD_SIZE), out_proj, preferred_element_type=jnp.float32)
    normed = rms_scale(mixed, ffn_gain).astype(jnp.bfloat16)
    routed = route_sum(normed, routes.reshape(-1).astype(jnp.int32), route_weights.reshape(-1), expert_gate, expert_up, expert_down)
    layer_out = (mixed + routed).astype(jnp.bfloat16)
    return (normed.reshape(SEQUENCE_COUNT, SEQUENCE_LENGTH, D), layer_out.reshape(SEQUENCE_COUNT, SEQUENCE_LENGTH, D))
```

```python
import functools

import jax
import jax.numpy as jnp
import numpy as np
from jax import lax
from jax.experimental import pallas as pl
from jax.experimental.pallas import tpu as pltpu
from jax.sharding import PartitionSpec as P

PLAIN = 64
ROT = 32
QK = PLAIN + ROT
VALUE = 64
GRID_W = 64
GROUP = 4

eps_norm = 1e-06
rope_base = 10000.0
clamp_limit = 7.0
glu_alpha = 1.702

F32 = jnp.float32
BF16 = jnp.bfloat16
MESH_ID = pl.DeviceIdType.MESH
VMEM_LIMIT = 60 * 1024 * 1024


def params(**kw):
    return pltpu.CompilerParams(vmem_limit_bytes=VMEM_LIMIT, **kw)


PLANE = 4
CHUNK = 512


def turn_tables(length):
    pair = np.arange(ROT) // 2
    quarter = ROT // 4
    frequency = (rope_base ** (-(2.0 * np.arange(quarter)) / (ROT // 2))).astype(np.float32)
    even = np.arange(ROT) % 2 == 0

    def part(places, mine, plain):
        angle = places.astype(np.float32)[:, None] * frequency[pair % quarter][None, :]
        cosine, sine = np.cos(angle.astype(np.float64)), np.sin(angle.astype(np.float64))
        tables = [cosine, np.where(even, -sine, 0.0), np.where(even, 0.0, sine)]
        wide = []
        for table, rest in zip(tables, plain):
            head = np.concatenate(
                [np.full((len(places), PLAIN), rest), np.where(mine, table, 0.0)], axis=1
            )
            wide += [head] * GROUP
        return np.concatenate(wide, axis=1).astype(np.float32)

    rows = part(np.arange(-(-length // GRID_W)), pair < quarter, (0.0, 0.0, 0.0))
    cols = part(np.arange(GRID_W), pair >= quarter, (1.0, 0.0, 0.0))
    return rows, cols


def exchange_kernel(count, dp_size, src, dst, send_sem, recv_sem, own_sem):
    me = lax.axis_index("sp") * dp_size + lax.axis_index("dp")
    barrier = pltpu.get_barrier_semaphore()

    def place(k):
        return lax.rem(me + k, count)

    def device(k):
        other = place(k)
        return (other // dp_size, lax.rem(other, dp_size))

    def greet(k, _):
        pl.semaphore_signal(barrier, inc=1, device_id=device(k), device_id_type=MESH_ID)
        return 0

    lax.fori_loop(1, count, greet, 0)
    own = pltpu.make_async_copy(src.at[me], dst.at[me], own_sem)
    own.start()
    pl.semaphore_wait(barrier, count - 1)

    def copy(k):
        return pltpu.make_async_remote_copy(
            src_ref=src.at[place(k)],
            dst_ref=dst.at[me],
            send_sem=send_sem.at[k],
            recv_sem=recv_sem.at[k],
            device_id=device(k),
            device_id_type=MESH_ID,
        )

    def start(k, _):
        copy(k).start()
        return 0

    def wait(k, _):
        copy(k).wait()
        return 0

    lax.fori_loop(1, count, start, 0)
    lax.fori_loop(1, count, wait, 0)
    own.wait()


def exchange(blocks, dp_size, collective_id):
    count = blocks.shape[0]
    if blocks.shape[1] % 16:
        return lax.all_to_all(blocks, ("sp", "dp"), split_axis=0, concat_axis=0, tiled=True)
    return pl.pallas_call(
        functools.partial(exchange_kernel, count, dp_size),
        out_shape=jax.ShapeDtypeStruct(blocks.shape, blocks.dtype),
        in_specs=[pl.BlockSpec(memory_space=pl.ANY)],
        out_specs=pl.BlockSpec(memory_space=pl.ANY),
        scratch_shapes=[
            pltpu.SemaphoreType.DMA((count,)),
            pltpu.SemaphoreType.DMA((count,)),
            pltpu.SemaphoreType.DMA,
        ],
        compiler_params=params(collective_id=collective_id, has_side_effects=True),
        name="expert_exchange",
    )(blocks)


def dot(a, b, dims=((1,), (0,))):
    return lax.dot_general(a, b, (dims, ((), ())), preferred_element_type=F32)


def lane_fold(x, op):
    parts = [x[:, i : i + 128] for i in range(0, x.shape[1], 128)]
    return functools.reduce(op, parts)


def attention_kernel(
    sp_size, experts, capacity,
    q_hbm, kup_hbm, vup_hbm, oproj_hbm, res_hbm,
    latent_ref, key_ref, lgain_ref, rows_ref, cols_ref, gain_ref, routes_ref,
    normed_ref, mixed_ref, out_ref, pick_ref,
    q, kup, vup, oproj, res, blocks, kt, lat, tab, qs, acc,
    scores_a, scores_b, top_a, top_b, load_sem, send_sem, recv_sem,
):
    sp = lax.axis_index("sp")
    dp = lax.axis_index("dp")
    tok = latent_ref.shape[0]
    width = latent_ref.shape[1]
    line = sp_size // PLANE
    z, p = sp // PLANE, lax.rem(sp, PLANE)
    x_near = z * PLANE + p + 1 - 2 * lax.rem(p, 2)
    y_near = z * PLANE + lax.rem(p + 2, PLANE)
    p_x, p_y = lax.rem(x_near, PLANE), lax.rem(y_near, PLANE)
    half_rot = ROT // 2

    def column(k):
        return lax.rem(z + k, line) * PLANE + p

    barrier = pltpu.get_barrier_semaphore()

    def greet(other):
        pl.semaphore_signal(barrier, inc=1, device_id=(other, dp), device_id_type=MESH_ID)

    def greet_line(k, _):
        greet(column(k))
        return 0

    lax.fori_loop(1, line, greet_line, 0)
    greet(x_near)
    greet(y_near)

    loads = [
        pltpu.make_async_copy(src, dst, load_sem.at[i])
        for i, (src, dst) in enumerate(
            [(q_hbm, q), (kup_hbm, kup), (vup_hbm, vup), (res_hbm, res), (oproj_hbm, oproj)]
        )
    ]
    for load in loads:
        load.start()

    grid_rows = tok // GRID_W
    lanes = GROUP * QK
    for s in range(grid_rows):
        wide = cols_ref[...] + rows_ref[pl.ds(sp * grid_rows + s, 1), :]
        for i in range(3):
            tab[i, s * GRID_W : (s + 1) * GRID_W, :] = wide[:, i * lanes : (i + 1) * lanes]

    def turn(x, width):
        return (
            x * tab[0, :, :width]
            + pltpu.roll(x, width - 1, 1) * tab[1, :, :width]
            + pltpu.roll(x, 1, 1) * tab[2, :, :width]
        )

    latent_float = latent_ref[...].astype(F32)
    square = jnp.mean(latent_float * latent_float, axis=1, keepdims=True)
    latent = latent_float * lax.rsqrt(square + eps_norm) * lgain_ref[...]
    blocks[sp, :tok, :] = latent.astype(BF16)
    key = key_ref[...].astype(F32)
    key = jnp.concatenate(
        [jnp.zeros((tok, PLAIN), F32), key, jnp.zeros((tok, 128 - QK), F32)], axis=1
    )
    key_columns = turn(key, 128).T.astype(BF16)
    blocks[sp, tok:, :tok] = key_columns[PLAIN : PLAIN + half_rot]
    blocks[sp, tok:, tok:] = key_columns[PLAIN + half_rot : QK]

    def copy(block, other, slot):
        return pltpu.make_async_remote_copy(
            src_ref=blocks.at[block],
            dst_ref=blocks.at[block],
            send_sem=send_sem.at[slot],
            recv_sem=recv_sem.at[block],
            device_id=(other, dp),
            device_id_type=MESH_ID,
        )

    def to_line(k):
        return copy(sp, column(k), k)

    def to_x(k):
        return copy(column(k), x_near, line + k)

    def to_y(k):
        return copy(column(k), y_near, 2 * line + k)

    def relay_y(k):
        return copy(k * PLANE + p_x, y_near, 3 * line + k)

    def relay_x(k):
        return copy(k * PLANE + p_y, x_near, 4 * line + k)

    def arrive(block):
        copy(block, sp, 0).wait_recv()

    def fill(block):
        at = pl.ds(pl.multiple_of(block * tok, tok), tok)
        lat[at, :] = blocks[block, :tok, :]
        kt[:width, at] = blocks[block, :tok, :].T
        kt[width : width + half_rot, at] = blocks[block, tok:, :tok]
        kt[width + half_rot :, at] = blocks[block, tok:, tok:]

    pl.semaphore_wait(barrier, line + 1)

    def start_line(k, _):
        to_line(k).start()
        return 0

    lax.fori_loop(1, line, start_line, 0)
    to_x(0).start()
    to_y(0).start()

    half = tok // 2
    rows = 2 * GROUP * half
    sets = q.shape[1] // lanes
    loads[0].wait()
    loads[1].wait()

    def prepare(j, _):
        x = q[:, pl.ds(pl.multiple_of(j * lanes, 128), lanes)].astype(F32)
        turned = turn(x, lanes) * (QK ** (-0.5))
        up = kup[:, pl.ds(pl.multiple_of(j * GROUP * PLAIN, 128), GROUP * PLAIN)]
        for i in range(GROUP):
            plain = turned[:, i * QK : i * QK + PLAIN].astype(BF16)
            absorbed = dot(plain, up[:, i * PLAIN : (i + 1) * PLAIN], ((1,), (1,))).astype(BF16)
            rotary = turned[:, i * QK + PLAIN : (i + 1) * QK].astype(BF16)
            at = slice(i * half, (i + 1) * half)
            for h in range(2):
                mine = slice(h * half, (h + 1) * half)
                qs[h * sets + j, at, :width] = absorbed[mine]
                qs[h * sets + j, at, width:] = rotary[mine]
        return 0

    early = sets // 4
    lax.fori_loop(0, early, prepare, 0)

    def pass_on(k, _):
        back = line - k
        block = column(back)
        arrive(block)
        to_x(back).start()
        to_y(back).start()
        return 0

    lax.fori_loop(1, line, pass_on, 0)
    lax.fori_loop(early, sets, prepare, 0)

    def fill_column(k, _):
        fill(k * PLANE + p)
        return 0

    lax.fori_loop(0, line, fill_column, 0)

    def relay(k, _):
        other = lax.rem(z + k, line)
        from_x, from_y = other * PLANE + p_x, other * PLANE + p_y
        arrive(from_x)

        @pl.when(lax.rem(other, 2) == 0)
        def _():
            relay_y(other).start()

        arrive(from_y)

        @pl.when(lax.rem(other, 2) == 1)
        def _():
            relay_x(other).start()

        fill(from_x)
        fill(from_y)
        return 0

    lax.fori_loop(0, line, relay, 0)

    def last(k, _):
        other = lax.rem(z + k, line)
        block = other * PLANE + (PLANE - 1 - p)
        arrive(block)
        fill(block)
        return 0

    lax.fori_loop(0, line, last, 0)

    length = lat.shape[0]
    chunk = min(CHUNK, length)
    groups = sets // 2
    for load in loads[2:]:
        load.wait()

    def score(g, scores, top):
        mine = qs[pl.ds(2 * g, 2)].reshape(rows, width + ROT)
        best = None
        for c in range(0, length, chunk):
            s = dot(mine, kt[:, c : c + chunk])
            scores[:, c : c + chunk] = s
            part = lane_fold(s, jnp.maximum)
            best = part if best is None else jnp.maximum(best, part)
        top[...] = best

    def weigh(g, scores, top):
        highest = jnp.max(top[...], axis=1, keepdims=True)
        total = context = None
        for c in range(0, length, chunk):
            w = jnp.exp(scores[:, c : c + chunk] - highest)
            part = lane_fold(w, jnp.add)
            seen = dot(w.astype(BF16), lat[c : c + chunk, :])
            total = part if total is None else total + part
            context = seen if context is None else context + seen
        context = (context / jnp.sum(total, axis=1, keepdims=True)).astype(BF16)
        spread = 2 * GROUP * VALUE
        at = pl.ds(pl.multiple_of(lax.rem(g, groups) * spread, spread), spread)
        up = vup[:, at]
        heads = [
            dot(context[i * half : (i + 1) * half], up[:, i * VALUE : (i + 1) * VALUE])
            for i in range(2 * GROUP)
        ]
        acc[...] += dot(jnp.concatenate(heads, axis=1).astype(BF16), oproj[at, :])

    def settle(h):
        at = pl.ds(pl.multiple_of(h * half, half), half)
        mixed = res[at, :].astype(F32) + acc[...]
        mixed_ref[at, :] = mixed
        mean = jnp.mean(mixed * mixed, axis=1, keepdims=True)
        normed_ref[at, :] = (mixed * lax.rsqrt(mean + eps_norm) * gain_ref[...]).astype(BF16)
        acc[...] = jnp.zeros_like(acc)

    acc[...] = jnp.zeros_like(acc)
    score(0, scores_a, top_a)

    def two(i, _):
        g = 2 * i
        weigh(g, scores_a, top_a)
        score(g + 1, scores_b, top_b)
        weigh(g + 1, scores_b, top_b)
        score(g + 2, scores_a, top_a)

        @pl.when(g + 2 == groups)
        def _():
            settle(0)

        return 0

    lax.fori_loop(0, groups - 1, two, 0)
    weigh(2 * groups - 2, scores_a, top_a)
    score(2 * groups - 1, scores_b, top_b)
    weigh(2 * groups - 1, scores_b, top_b)
    settle(1)

    slots = experts * capacity
    expert_lane = lax.broadcasted_iota(jnp.int32, (tok, experts), 1)
    slot_lane = lax.broadcasted_iota(jnp.int32, (tok, slots), 1)
    earlier = (
        lax.broadcasted_iota(jnp.int32, (tok, tok), 1)
        < lax.broadcasted_iota(jnp.int32, (tok, tok), 0)
    ).astype(BF16)
    routes = routes_ref[...]
    taken = jnp.zeros((1, experts), F32)
    picks = []
    for k in range(routes.shape[1]):
        expert = routes[:, k : k + 1]
        named = (expert_lane == expert).astype(F32)
        before = dot(earlier, named.astype(BF16)) + taken
        rank = jnp.sum(before * named, axis=1, keepdims=True)
        slot = expert * capacity + rank.astype(jnp.int32)
        pick = (slot_lane == slot).astype(F32)
        pick_ref[k * tok : (k + 1) * tok, :] = pick.astype(BF16)
        picks.append(pick)
        taken = taken + jnp.sum(named, axis=0, keepdims=True)
    spread = functools.reduce(jnp.add, picks).T.astype(BF16)
    out_ref[...] = dot(spread, normed_ref[...]).astype(BF16)

    def sent(k, _):
        to_x(k).wait_send()
        to_y(k).wait_send()

        @pl.when(k > 0)
        def _():
            to_line(k).wait_send()

        @pl.when(lax.rem(k, 2) == 0)
        def _():
            relay_y(k).wait_send()

        @pl.when(lax.rem(k, 2) == 1)
        def _():
            relay_x(k).wait_send()

        return 0

    lax.fori_loop(0, line, sent, 0)


def attention(q, latent, key, lgain, kup, vup, oproj, res, gain, routes, sp_size, experts, capacity):
    tok, d = res.shape
    width = latent.shape[1]
    length = sp_size * tok
    slots = experts * capacity
    picks = routes.shape[1] * tok
    lanes = GROUP * QK
    sets = q.shape[1] // lanes
    rows = GROUP * tok
    row_table, col_table = turn_tables(length)
    far = pl.BlockSpec(memory_space=pl.ANY)
    near = pl.BlockSpec(memory_space=pltpu.VMEM)
    return pl.pallas_call(
        functools.partial(attention_kernel, sp_size, experts, capacity),
        in_specs=[far] * 5 + [near] * 7,
        out_specs=[near] * 4,
        out_shape=[
            jax.ShapeDtypeStruct((tok, d), BF16),
            jax.ShapeDtypeStruct((tok, d), F32),
            jax.ShapeDtypeStruct((slots, d), BF16),
            jax.ShapeDtypeStruct((picks, slots), BF16),
        ],
        scratch_shapes=[
            pltpu.VMEM(q.shape, BF16),
            pltpu.VMEM(kup.shape, BF16),
            pltpu.VMEM(vup.shape, BF16),
            pltpu.VMEM(oproj.shape, BF16),
            pltpu.VMEM(res.shape, BF16),
            pltpu.VMEM((sp_size, tok + ROT // 2, width), BF16),
            pltpu.VMEM((width + ROT, length), BF16),
            pltpu.VMEM((length, width), BF16),
            pltpu.VMEM((3, tok, lanes), F32),
            pltpu.VMEM((2 * sets, rows // 2, width + ROT), BF16),
            pltpu.VMEM((tok // 2, d), F32),
            pltpu.VMEM((rows, length), F32),
            pltpu.VMEM((rows, length), F32),
            pltpu.VMEM((rows, 128), F32),
            pltpu.VMEM((rows, 128), F32),
            pltpu.SemaphoreType.DMA((5,)),
            pltpu.SemaphoreType.DMA((5 * sp_size // PLANE,)),
            pltpu.SemaphoreType.DMA((sp_size,)),
        ],
        compiler_params=params(collective_id=0, has_side_effects=True),
        name="attention",
    )(q, kup, vup, oproj, res, latent, key, lgain, row_table, col_table, gain, routes)


def expert_kernel(x_ref, gate_ref, up_ref, down_ref, out_ref, acc):
    step = pl.program_id(0)
    x = x_ref[...]
    gate = jnp.minimum(dot(x, gate_ref[...]), clamp_limit)
    up = jnp.clip(dot(x, up_ref[...]), -clamp_limit, clamp_limit)
    hidden = (gate * jax.nn.sigmoid(glu_alpha * gate) * (up + 1.0)).astype(BF16)
    part = dot(hidden, down_ref[...])

    @pl.when(step == 0)
    def _():
        acc[...] = part

    @pl.when(step > 0)
    def _():
        acc[...] += part

    @pl.when(step == pl.num_programs(0) - 1)
    def _():
        out_ref[...] = acc[...].astype(BF16)


def expert_rows(x, gate_w, up_w, down_w):
    rows, d = x.shape
    ff = gate_w.shape[1]
    tile = 256
    return pl.pallas_call(
        expert_kernel,
        grid=(ff // tile,),
        in_specs=[
            pl.BlockSpec((rows, d), lambda f: (0, 0)),
            pl.BlockSpec((d, tile), lambda f: (0, f)),
            pl.BlockSpec((d, tile), lambda f: (0, f)),
            pl.BlockSpec((tile, d), lambda f: (f, 0)),
        ],
        out_specs=pl.BlockSpec((rows, d), lambda f: (0, 0)),
        out_shape=jax.ShapeDtypeStruct((rows, d), BF16),
        scratch_shapes=[pltpu.VMEM((rows, d), F32)],
        compiler_params=params(dimension_semantics=("arbitrary",)),
        name="experts",
    )(x, gate_w, up_w, down_w)


def combine_kernel(pick_ref, back_ref, weight_ref, mixed_ref, out_ref):
    tok = mixed_ref.shape[0]
    rows = dot(pick_ref[...], back_ref[...])
    total = mixed_ref[...]
    routed = None
    for k in range(weight_ref.shape[1]):
        term = rows[k * tok : (k + 1) * tok] * weight_ref[:, k : k + 1]
        routed = term if routed is None else routed + term
    out_ref[...] = (total + routed).astype(BF16)


def combine(pick, back, weight, mixed):
    tok, d = mixed.shape
    slots = back.shape[0]
    tile = 512
    return pl.pallas_call(
        combine_kernel,
        grid=(d // tile,),
        in_specs=[
            pl.BlockSpec(pick.shape, lambda j: (0, 0)),
            pl.BlockSpec((slots, tile), lambda j: (0, j)),
            pl.BlockSpec(weight.shape, lambda j: (0, 0)),
            pl.BlockSpec((tok, tile), lambda j: (0, j)),
        ],
        out_specs=pl.BlockSpec((tok, tile), lambda j: (0, j)),
        out_shape=jax.ShapeDtypeStruct((tok, d), BF16),
        compiler_params=params(dimension_semantics=("arbitrary",)),
        name="combine",
    )(pick, back, weight, mixed)


def local(
    queries,
    kv_latent,
    rope_key,
    latent_norm_gain,
    key_up_weight,
    value_up_weight,
    out_proj,
    residual,
    ffn_gain,
    routes,
    route_weights,
    expert_gate,
    expert_up,
    expert_down,
):
    tok = queries.shape[1]
    d = residual.shape[2]
    topk = routes.shape[2]
    sp_size = lax.axis_size("sp")
    dp_size = lax.axis_size("dp")
    experts = sp_size * dp_size
    capacity = max(2, 2 * tok * topk // experts)
    normed, mixed, outgoing, pick = attention(
        queries[0], kv_latent[0], rope_key[0], latent_norm_gain[None], key_up_weight,
        value_up_weight, out_proj, residual[0], ffn_gain[None], routes[0],
        sp_size, experts, capacity,
    )
    blocks = outgoing.reshape(experts, capacity, d)
    slot_rows = exchange(blocks, dp_size, 1).reshape(experts * capacity, d)
    expert_out = expert_rows(slot_rows, expert_gate[0], expert_up[0], expert_down[0])
    back = exchange(expert_out.reshape(blocks.shape), dp_size, 2)
    layer_out = combine(pick, back.reshape(experts * capacity, d), route_weights[0], mixed)
    return (normed[None], layer_out[None])


def solution(mesh):
    in_specs = (
        P("dp", "sp", None),
        P("dp", "sp", None),
        P("dp", "sp", None),
        P(),
        P(),
        P(),
        P(),
        P("dp", "sp", None),
        P(),
        P("dp", "sp", None),
        P("dp", "sp", None),
        P(("sp", "dp"), None, None),
        P(("sp", "dp"), None, None),
        P(("sp", "dp"), None, None),
    )
    out_specs = (P("dp", "sp", None), P("dp", "sp", None))
    return jax.shard_map(local, mesh=mesh, in_specs=in_specs, out_specs=out_specs, check_vma=False)
```

```python
import functools
import types

import jax
import jax.numpy as jnp
import numpy as np
from jax import lax
from jax.experimental import pallas as pl
from jax.experimental.pallas import tpu as pltpu
from jax.sharding import PartitionSpec as P

PLAIN = 64
ROT = 32
QK = PLAIN + ROT
VALUE = 64
GRID_W = 64
GROUP = 4

eps_norm = 1e-06
rope_base = 10000.0
clamp_limit = 7.0
glu_alpha = 1.702

F32 = jnp.float32
BF16 = jnp.bfloat16
MESH_ID = pl.DeviceIdType.MESH
VMEM_LIMIT = 60 * 1024 * 1024
LAYER_VMEM = 63 * 1024 * 1024 + 900 * 1024


def params(**kw):
    return pltpu.CompilerParams(**{'vmem_limit_bytes': VMEM_LIMIT, **kw})


PLANE = 4
CHUNK = 512


def turn_tables(length):
    pair = np.arange(ROT) // 2
    quarter = ROT // 4
    frequency = (rope_base ** (-(2.0 * np.arange(quarter)) / (ROT // 2))).astype(np.float32)
    even = np.arange(ROT) % 2 == 0

    def part(places, mine, plain):
        angle = places.astype(np.float32)[:, None] * frequency[pair % quarter][None, :]
        cosine, sine = np.cos(angle.astype(np.float64)), np.sin(angle.astype(np.float64))
        tables = [cosine, np.where(even, -sine, 0.0), np.where(even, 0.0, sine)]
        wide = []
        for table, rest in zip(tables, plain):
            head = np.concatenate(
                [np.full((len(places), PLAIN), rest), np.where(mine, table, 0.0)], axis=1
            )
            wide += [head] * GROUP
        return np.concatenate(wide, axis=1).astype(np.float32)

    rows = part(np.arange(-(-length // GRID_W)), pair < quarter, (0.0, 0.0, 0.0))
    cols = part(np.arange(GRID_W), pair >= quarter, (1.0, 0.0, 0.0))
    return rows, cols


def exchange_kernel(count, dp_size, src, dst, send_sem, recv_sem, own_sem):
    me = lax.axis_index("sp") * dp_size + lax.axis_index("dp")
    barrier = pltpu.get_barrier_semaphore()

    def place(k):
        return lax.rem(me + k, count)

    def device(k):
        other = place(k)
        return (other // dp_size, lax.rem(other, dp_size))

    def greet(k, _):
        pl.semaphore_signal(barrier, inc=1, device_id=device(k), device_id_type=MESH_ID)
        return 0

    lax.fori_loop(1, count, greet, 0)
    own = pltpu.make_async_copy(src.at[me], dst.at[me], own_sem)
    own.start()
    pl.semaphore_wait(barrier, count - 1)

    def copy(k):
        return pltpu.make_async_remote_copy(
            src_ref=src.at[place(k)],
            dst_ref=dst.at[me],
            send_sem=send_sem.at[k],
            recv_sem=recv_sem.at[k],
            device_id=device(k),
            device_id_type=MESH_ID,
        )

    def start(k, _):
        copy(k).start()
        return 0

    def wait(k, _):
        copy(k).wait()
        return 0

    lax.fori_loop(1, count, start, 0)
    lax.fori_loop(1, count, wait, 0)
    own.wait()


def exchange(blocks, dp_size, collective_id):
    count = blocks.shape[0]
    if blocks.shape[1] % 16:
        return lax.all_to_all(blocks, ("sp", "dp"), split_axis=0, concat_axis=0, tiled=True)
    return pl.pallas_call(
        functools.partial(exchange_kernel, count, dp_size),
        out_shape=jax.ShapeDtypeStruct(blocks.shape, blocks.dtype),
        in_specs=[pl.BlockSpec(memory_space=pl.ANY)],
        out_specs=pl.BlockSpec(memory_space=pl.ANY),
        scratch_shapes=[
            pltpu.SemaphoreType.DMA((count,)),
            pltpu.SemaphoreType.DMA((count,)),
            pltpu.SemaphoreType.DMA,
        ],
        compiler_params=params(collective_id=collective_id, has_side_effects=True),
        name="expert_exchange",
    )(blocks)


def dot(a, b, dims=((1,), (0,))):
    return lax.dot_general(a, b, (dims, ((), ())), preferred_element_type=F32)


def lane_fold(x, op):
    parts = [x[:, i : i + 128] for i in range(0, x.shape[1], 128)]
    return functools.reduce(op, parts)


def layer_kernel(names, sizes, *refs):
    r = types.SimpleNamespace(**dict(zip(names, refs)))
    sp_size, dp_size, experts, capacity, fused = sizes
    sp = lax.axis_index("sp")
    dp = lax.axis_index("dp")
    tok, width = r.latent.shape
    d = r.res.shape[1]
    topk = r.routes.shape[0]
    length = sp_size * tok
    line = sp_size // PLANE
    z, p = sp // PLANE, lax.rem(sp, PLANE)
    x_near = z * PLANE + p + 1 - 2 * lax.rem(p, 2)
    y_near = z * PLANE + lax.rem(p + 2, PLANE)
    p_x, p_y = lax.rem(x_near, PLANE), lax.rem(y_near, PLANE)
    half_rot = ROT // 2
    half = tok // 2
    rows = 2 * GROUP * half
    lanes = GROUP * QK
    sets = r.q.shape[1] // lanes
    groups = sets // 2
    tile = min(512, d)
    me = sp * dp_size + dp

    def column(k):
        return lax.rem(z + k, line) * PLANE + p

    barrier = pltpu.get_barrier_semaphore()

    def greet(place, other_dp):
        pl.semaphore_signal(barrier, inc=1, device_id=(place, other_dp), device_id_type=MESH_ID)

    if fused:
        greeted = sp_size * dp_size - 1

        def greet_other(k, _):
            other = lax.rem(me + k, sp_size * dp_size)
            greet(other // dp_size, lax.rem(other, dp_size))
            return 0

        lax.fori_loop(1, greeted + 1, greet_other, 0)
    else:
        greeted = line + 1

        def greet_line(k, _):
            greet(column(k), dp)
            return 0

        lax.fori_loop(1, line, greet_line, 0)
        greet(x_near, dp)
        greet(y_near, dp)

    loaded = [
        "latent", "key", "lgain", "row_table", "col_table", "routes",
        "q", "kup", "vup", "res", "oproj", "gain",
    ]
    if fused:
        loaded += ["weights", "gate", "up", "down"]
    loads = {
        name: pltpu.make_async_copy(getattr(r, name + "_hbm"), getattr(r, name), r.load_sem.at[i])
        for i, name in enumerate(loaded)
    }
    for name in loaded:
        loads[name].start()
    for name in loaded[:6]:
        loads[name].wait()

    grid_rows = tok // GRID_W
    for s in range(grid_rows):
        wide = r.col_table[...] + r.row_table[pl.ds(sp * grid_rows + s, 1), :]
        for i in range(3):
            r.tab[i, s * GRID_W : (s + 1) * GRID_W, :] = wide[:, i * lanes : (i + 1) * lanes]

    def turn(x, wide):
        return (
            x * r.tab[0, :, :wide]
            + pltpu.roll(x, wide - 1, 1) * r.tab[1, :, :wide]
            + pltpu.roll(x, 1, 1) * r.tab[2, :, :wide]
        )

    blocks = r.blocks
    latent_float = r.latent[...].astype(F32)
    square = jnp.mean(latent_float * latent_float, axis=1, keepdims=True)
    latent = latent_float * lax.rsqrt(square + eps_norm) * r.lgain[...]
    blocks[sp, :tok, :] = latent.astype(BF16)
    key = r.key[...].astype(F32)
    key = jnp.concatenate(
        [jnp.zeros((tok, PLAIN), F32), key, jnp.zeros((tok, 128 - QK), F32)], axis=1
    )
    key_columns = turn(key, 128).T.astype(BF16)
    blocks[sp, tok:, :tok] = key_columns[PLAIN : PLAIN + half_rot]
    blocks[sp, tok:, tok:] = key_columns[PLAIN + half_rot : QK]
    if fused:
        r.line_routes[z] = jnp.concatenate(
            [r.routes[...], jnp.zeros((8 - topk, tok), jnp.int32)], axis=0
        )

    def remote(src, dst, send, recv, place, other_dp):
        return pltpu.make_async_remote_copy(
            src_ref=src,
            dst_ref=dst,
            send_sem=send,
            recv_sem=recv,
            device_id=(place, other_dp),
            device_id_type=MESH_ID,
        )

    def copy(block, other, slot):
        block = blocks.at[block], r.recv_sem.at[block]
        return remote(block[0], block[0], r.send_sem.at[slot], block[1], other, dp)

    def to_line(k):
        return copy(sp, column(k), k)

    def to_x(k):
        return copy(column(k), x_near, line + k)

    def to_y(k):
        return copy(column(k), y_near, 2 * line + k)

    def relay_y(k):
        return copy(k * PLANE + p_x, y_near, 3 * line + k)

    def relay_x(k):
        return copy(k * PLANE + p_y, x_near, 4 * line + k)

    def arrive(block):
        copy(block, sp, 0).wait_recv()

    def routes_to(k, back=False):
        place = lax.rem(z + line - k, line) if back else z
        ref = r.line_routes.at[place]
        return remote(
            ref, ref, r.route_send.at[k], r.route_recv.at[place], column(k), dp
        )

    def fill(block):
        at = pl.ds(pl.multiple_of(block * tok, tok), tok)
        r.lat[at, :] = blocks[block, :tok, :]
        r.kt[:width, at] = blocks[block, :tok, :].T
        r.kt[width : width + half_rot, at] = blocks[block, tok:, :tok]
        r.kt[width + half_rot :, at] = blocks[block, tok:, tok:]

    loads["q"].wait()
    loads["kup"].wait()

    def prepare(j, _):
        x = r.q[:, pl.ds(pl.multiple_of(j * lanes, 128), lanes)].astype(F32)
        turned = turn(x, lanes) * (QK ** (-0.5))
        up = r.kup[:, pl.ds(pl.multiple_of(j * GROUP * PLAIN, 128), GROUP * PLAIN)]
        for i in range(GROUP):
            plain = turned[:, i * QK : i * QK + PLAIN].astype(BF16)
            absorbed = dot(plain, up[:, i * PLAIN : (i + 1) * PLAIN], ((1,), (1,))).astype(BF16)
            rotary = turned[:, i * QK + PLAIN : (i + 1) * QK].astype(BF16)
            at = slice(i * half, (i + 1) * half)
            for h in range(2):
                mine = slice(h * half, (h + 1) * half)
                r.qs[h * sets + j, at, :width] = absorbed[mine]
                r.qs[h * sets + j, at, width:] = rotary[mine]
        return 0

    pl.semaphore_wait(barrier, greeted)
    to_x(0).start()
    to_y(0).start()

    def start_line(k, _):
        to_line(k).start()
        if fused:
            routes_to(k).start()
        return 0

    lax.fori_loop(1, line, start_line, 0)
    early = sets // 4
    lax.fori_loop(0, early, prepare, 0)

    def pass_on(k, _):
        back = line - k
        arrive(column(back))
        to_x(back).start()
        to_y(back).start()
        return 0

    lax.fori_loop(1, line, pass_on, 0)
    lax.fori_loop(early, sets, prepare, 0)

    def fill_column(k, _):
        fill(k * PLANE + p)
        return 0

    lax.fori_loop(0, line, fill_column, 0)

    def relay(k, _):
        other = lax.rem(z + k, line)
        from_x, from_y = other * PLANE + p_x, other * PLANE + p_y
        arrive(from_x)

        @pl.when(lax.rem(other, 2) == 0)
        def _():
            relay_y(other).start()

        arrive(from_y)

        @pl.when(lax.rem(other, 2) == 1)
        def _():
            relay_x(other).start()

        fill(from_x)
        fill(from_y)
        return 0

    lax.fori_loop(0, line, relay, 0)

    def last(k, _):
        block = lax.rem(z + k, line) * PLANE + (PLANE - 1 - p)
        arrive(block)
        fill(block)
        return 0

    lax.fori_loop(0, line, last, 0)
    for name in ("vup", "res", "oproj", "gain"):
        loads[name].wait()

    chunk = min(CHUNK, length)
    buffers = [(r.scores_a, r.top_a), (r.scores_b, r.top_b)]

    def step(weighed, scored, slot):
        if scored is not None:
            mine = r.qs[pl.ds(2 * scored, 2)].reshape(rows, width + ROT)
            new_scores, new_top = buffers[slot]
        if weighed is not None:
            scores, top = buffers[1 - slot]
            highest = jnp.max(top[...], axis=1, keepdims=True)
        best = total = context = None
        for c in range(0, length, chunk):
            at = slice(c, c + chunk)
            if weighed is not None:
                w = jnp.exp(scores[:, at] - highest)
                part = lane_fold(w, jnp.add)
                seen = dot(w.astype(BF16), r.lat[at, :])
                total = part if total is None else total + part
                context = seen if context is None else context + seen
            if scored is not None:
                fresh = dot(mine, r.kt[:, at])
                new_scores[:, at] = fresh
                part = lane_fold(fresh, jnp.maximum)
                best = part if best is None else jnp.maximum(best, part)
        if scored is not None:
            new_top[...] = best
        if weighed is not None:
            context = context / jnp.sum(total, axis=1, keepdims=True)
            r.context[lax.rem(weighed, groups)] = context.astype(BF16)

    def settle(h):
        at = slice(h * half, (h + 1) * half)
        for j in range(groups):
            heads = [
                dot(
                    r.context[j, i * half : (i + 1) * half],
                    r.vup[:, (j * 2 * GROUP + i) * VALUE : (j * 2 * GROUP + i + 1) * VALUE],
                )
                for i in range(2 * GROUP)
            ]
            spread = 2 * GROUP * VALUE
            r.heads[:, j * spread : (j + 1) * spread] = jnp.concatenate(heads, axis=1).astype(BF16)
        square = jnp.zeros((half, 128), F32)
        for n in range(0, d, tile):
            part = r.res[at, n : n + tile].astype(F32) + dot(r.heads[...], r.oproj[:, n : n + tile])
            r.mixed[at, n : n + tile] = part
            square = square + lane_fold(part * part, jnp.add)
        scale = lax.rsqrt(jnp.sum(square, axis=1, keepdims=True) / d + eps_norm)
        normed = (r.mixed[at, :] * scale * r.gain[...]).astype(BF16)
        r.normed[at, :] = normed
        if fused:
            r.tokens[z, at, :] = normed

    def ship(block, h, up):
        ref = r.tokens.at[block, pl.ds(h * half, half), :]
        slot = ((2 if up else 0) + h) * line + block
        return remote(
            ref, ref, r.ship_send.at[slot], r.ship_recv.at[h * line + block],
            sp + PLANE if up else sp - PLANE, dp,
        )

    def ship_both(block, h, act):
        @pl.when((block <= z) & (z + 1 < line))
        def _():
            act(ship(block, h, True))

        @pl.when((block >= z) & (z > 0))
        def _():
            act(ship(block, h, False))

    def start(c):
        c.start()

    def forward(block, h):
        ship(block, h, True).wait_recv()
        ship_both(block, h, start)

    step(None, 0, 0)

    def two(i, _):
        g = 2 * i
        step(g, g + 1, 1)
        step(g + 1, g + 2, 0)

        @pl.when(g + 2 == groups)
        def _():
            settle(0)
            if fused:
                ship_both(z, 0, start)

        return 0

    lax.fori_loop(0, groups - 1, two, 0)
    step(2 * groups - 2, 2 * groups - 1, 1)
    if fused:

        @pl.when(z > 0)
        def _():
            forward(z - 1, 0)

        @pl.when(z + 1 < line)
        def _():
            forward(z + 1, 0)

    step(2 * groups - 1, None, 0)
    settle(1)

    expert_lane = lax.broadcasted_iota(jnp.int32, (tok, experts), 1)
    slot_lane = lax.broadcasted_iota(jnp.int32, (tok, experts * capacity), 1)
    place_a = lax.broadcasted_iota(jnp.int32, (tok, tok), 0)
    place_b = lax.broadcasted_iota(jnp.int32, (tok, tok), 1)

    def columns(part):
        rest = jnp.zeros((tok - topk, tok), F32)
        return jnp.concatenate([part.astype(F32), rest], axis=0).T

    def pick_rows():
        routes = columns(r.routes[...])
        earlier = (place_b < place_a).astype(BF16)
        taken = jnp.zeros((1, experts), F32)
        picks = []
        for k in range(topk):
            expert = routes[:, k : k + 1].astype(jnp.int32)
            named = (expert_lane == expert).astype(F32)
            before = dot(earlier, named.astype(BF16)) + taken
            rank = jnp.sum(before * named, axis=1, keepdims=True)
            slot = expert * capacity + rank.astype(jnp.int32)
            pick = (slot_lane == slot).astype(F32)
            r.pick[k * tok : (k + 1) * tok, :] = pick.astype(BF16)
            picks.append(pick)
            taken = taken + jnp.sum(named, axis=0, keepdims=True)
        return picks

    if fused:
        ship_both(z, 1, start)
        near = PLANE * dp_size
        mine = p * dp_size + dp
        local_row = lax.broadcasted_iota(jnp.int32, (near, tok), 0)
        slot_row = lax.broadcasted_iota(jnp.int32, (near * capacity, tok), 0)

        def wait_routes(k, _):
            routes_to(k, True).wait_recv()
            return 0

        lax.fori_loop(1, line, wait_routes, 0)

        def give(block, other):
            return remote(
                r.stage.at[block, other], r.inbox.at[block, mine],
                r.give_send.at[block * near + other], r.give_recv.at[block * near + mine],
                z * PLANE + other // dp_size, lax.rem(other, dp_size),
            )

        def given(block, other):
            return remote(
                r.stage.at[block, other], r.inbox.at[block, other],
                r.give_send.at[block * near + other], r.give_recv.at[block * near + other],
                z * PLANE + other // dp_size, lax.rem(other, dp_size),
            )

        def dispatch(block):
            later = (place_a < place_b).astype(F32)
            taken = jnp.zeros((near, 1), F32)
            spread = None
            for k in range(topk):
                route = r.line_routes[block, k : k + 1, :] - z * near
                named = (local_row == route).astype(F32)
                before = dot(named, later) + taken
                slot = local_row.astype(F32) * capacity + before + 1.0
                slot = jnp.sum(named * slot, axis=0, keepdims=True).astype(jnp.int32) - 1
                pick = slot_row == slot
                spread = pick if spread is None else spread | pick
                taken = taken + jnp.sum(named, axis=1, keepdims=True)
            spread = spread.astype(F32).astype(BF16)
            for n in range(0, d, tile):
                part = dot(spread, r.tokens[block, :, n : n + tile]).astype(BF16)
                r.stage[block, :, :, n : n + tile] = part.reshape(near, capacity, tile)
            r.inbox[block, mine] = r.stage[block, mine]

            def send(k, _):
                give(block, lax.rem(mine + k, near)).start()
                return 0

            lax.fori_loop(1, near, send, 0)

        def answer(block, other):
            return remote(
                r.outbox.at[block, other], r.back.at[me],
                r.back_send.at[block * near + other], r.back_recv.at[me],
                block * PLANE + other // dp_size, lax.rem(other, dp_size),
            )

        def answer_all(block, act):
            def one(other, _):
                @pl.when((block != z) | (other != mine))
                def _():
                    act(answer(block, other))

                return 0

            lax.fori_loop(0, near, one, 0)

        def expert(block):
            def wait(k, _):
                given(block, lax.rem(mine + k, near)).wait_recv()
                return 0

            lax.fori_loop(1, near, wait, 0)
            x = r.inbox[block].reshape(near * capacity, d)
            for n in range(0, r.gate.shape[1], 256):
                at = slice(n, n + 256)
                gate = jnp.minimum(dot(x, r.gate[:, at]), clamp_limit)
                up = jnp.clip(dot(x, r.up[:, at]), -clamp_limit, clamp_limit)
                hidden = gate * jax.nn.sigmoid(glu_alpha * gate) * (up + 1.0)
                r.hidden[:, at] = hidden.astype(BF16)
            for n in range(0, d, tile):
                part = dot(r.hidden[...], r.down[:, n : n + tile]).astype(BF16)
                r.outbox[block, :, :, n : n + tile] = part.reshape(near, capacity, tile)

            @pl.when(block == z)
            def _():
                r.back[me] = r.outbox[block, mine]

            answer_all(block, start)

        for name in ("weights", "gate", "up", "down"):
            loads[name].wait()

        def at_hop(t, act):
            block = z + jnp.where(lax.rem(t, 2) == 1, -((t + 1) // 2), t // 2)

            @pl.when((block >= 0) & (block < line))
            def _():
                act(block)

        lag = 2
        hops = 2 * line - 1

        def hop(t, _):
            def bring(block):
                @pl.when(t > 2)
                def _():
                    forward(block, 0)

                @pl.when(t > 0)
                def _():
                    forward(block, 1)

                dispatch(block)

            @pl.when(t < hops)
            def _():
                at_hop(t, bring)

            @pl.when(t >= lag)
            def _():
                at_hop(t - lag, expert)

            return 0

        lax.fori_loop(0, hops + lag, hop, 0)
        pick_rows()
        weights = columns(r.weights[...])

        def wait_back(k, _):
            other = lax.rem(me + k, experts)
            remote(
                r.outbox.at[0, 0], r.back.at[other], r.back_send.at[0], r.back_recv.at[other], sp, dp
            ).wait_recv()
            return 0

        lax.fori_loop(1, experts, wait_back, 0)
        for n in range(0, d, tile):
            back = r.back[:, :, n : n + tile].reshape(experts * capacity, tile)
            picked = dot(r.pick[...], back)
            routed = None
            for k in range(topk):
                term = picked[k * tok : (k + 1) * tok] * weights[:, k : k + 1]
                routed = term if routed is None else routed + term
            r.out[:, n : n + tile] = (r.mixed[:, n : n + tile] + routed).astype(BF16)

        def finish(block, _):
            def drain(c):
                c.wait_send()

            for h in range(2):
                ship_both(block, h, drain)
            answer_all(block, drain)

            def sent_all(k, _):
                give(block, lax.rem(mine + k, near)).wait_send()
                return 0

            lax.fori_loop(1, near, sent_all, 0)
            return 0

        lax.fori_loop(0, line, finish, 0)
    else:
        spread = functools.reduce(jnp.add, pick_rows()).T.astype(BF16)
        r.slots[...] = dot(spread, r.normed[...]).astype(BF16)

    def sent(k, _):
        to_x(k).wait_send()
        to_y(k).wait_send()

        @pl.when(k > 0)
        def _():
            to_line(k).wait_send()
            if fused:
                routes_to(k).wait_send()

        @pl.when(lax.rem(k, 2) == 0)
        def _():
            relay_y(k).wait_send()

        @pl.when(lax.rem(k, 2) == 1)
        def _():
            relay_x(k).wait_send()

        return 0

    lax.fori_loop(0, line, sent, 0)


def layer(operands, sp_size, dp_size, capacity, fused):
    tok, d = operands["res"].shape
    width = operands["latent"].shape[1]
    ff = operands["gate"].shape[1]
    topk = operands["routes"].shape[0]
    experts = sp_size * dp_size
    length = sp_size * tok
    line = sp_size // PLANE
    near = PLANE * dp_size
    slots = experts * capacity
    lanes = GROUP * QK
    sets = operands["q"].shape[1] // lanes
    rows = GROUP * tok
    if not fused:
        operands = {k: v for k, v in operands.items() if k not in ("weights", "gate", "up", "down")}
    inputs = list(operands)
    vmem, dma = pltpu.VMEM, pltpu.SemaphoreType.DMA
    scratch = {name: vmem(operands[name].shape, operands[name].dtype) for name in inputs}
    scratch.update(
        blocks=vmem((sp_size, tok + ROT // 2, width), BF16),
        kt=vmem((width + ROT, length), BF16),
        lat=vmem((length, width), BF16),
        tab=vmem((3, tok, lanes), F32),
        qs=vmem((2 * sets, rows // 2, width + ROT), BF16),
        context=vmem((sets // 2, rows, width), BF16),
        heads=vmem((tok // 2, sets * GROUP * VALUE), BF16),
        scores_a=vmem((rows, length), F32),
        scores_b=vmem((rows, length), F32),
        top_a=vmem((rows, 128), F32),
        top_b=vmem((rows, 128), F32),
        load_sem=dma((len(inputs),)),
        send_sem=dma((5 * line,)),
        recv_sem=dma((sp_size,)),
    )
    outputs = {"normed": jax.ShapeDtypeStruct((tok, d), BF16)}
    if fused:
        outputs["out"] = jax.ShapeDtypeStruct((tok, d), BF16)
        scratch.update(
            mixed=vmem((tok, d), F32),
            pick=vmem((topk * tok, slots), BF16),
            line_routes=vmem((line, 8, tok), jnp.int32),
            tokens=vmem((line, tok, d), BF16),
            stage=vmem((line, near, capacity, d), BF16),
            inbox=vmem((line, near, capacity, d), BF16),
            outbox=vmem((line, near, capacity, d), BF16),
            back=vmem((experts, capacity, d), BF16),
            hidden=vmem((near * capacity, ff), BF16),
            route_send=dma((line,)),
            route_recv=dma((line,)),
            ship_send=dma((4 * line,)),
            ship_recv=dma((2 * line,)),
            give_send=dma((line * near,)),
            give_recv=dma((line * near,)),
            back_send=dma((line * near,)),
            back_recv=dma((experts,)),
        )
    else:
        outputs["mixed"] = jax.ShapeDtypeStruct((tok, d), F32)
        outputs["slots"] = jax.ShapeDtypeStruct((slots, d), BF16)
        outputs["pick"] = jax.ShapeDtypeStruct((topk * tok, slots), BF16)
    names = [name + "_hbm" for name in inputs] + list(outputs) + list(scratch)
    return pl.pallas_call(
        functools.partial(layer_kernel, names, (sp_size, dp_size, experts, capacity, fused)),
        in_specs=[pl.BlockSpec(memory_space=pl.ANY)] * len(inputs),
        out_specs=[pl.BlockSpec(memory_space=pltpu.VMEM)] * len(outputs),
        out_shape=list(outputs.values()),
        scratch_shapes=list(scratch.values()),
        compiler_params=params(
            collective_id=0, has_side_effects=True, vmem_limit_bytes=LAYER_VMEM
        ),
        name="layer",
    )(*operands.values())


def expert_kernel(x_ref, gate_ref, up_ref, down_ref, out_ref, acc):
    step = pl.program_id(0)
    x = x_ref[...]
    gate = jnp.minimum(dot(x, gate_ref[...]), clamp_limit)
    up = jnp.clip(dot(x, up_ref[...]), -clamp_limit, clamp_limit)
    hidden = (gate * jax.nn.sigmoid(glu_alpha * gate) * (up + 1.0)).astype(BF16)
    part = dot(hidden, down_ref[...])

    @pl.when(step == 0)
    def _():
        acc[...] = part

    @pl.when(step > 0)
    def _():
        acc[...] += part

    @pl.when(step == pl.num_programs(0) - 1)
    def _():
        out_ref[...] = acc[...].astype(BF16)


def expert_rows(x, gate_w, up_w, down_w):
    rows, d = x.shape
    ff = gate_w.shape[1]
    tile = 256
    return pl.pallas_call(
        expert_kernel,
        grid=(ff // tile,),
        in_specs=[
            pl.BlockSpec((rows, d), lambda f: (0, 0)),
            pl.BlockSpec((d, tile), lambda f: (0, f)),
            pl.BlockSpec((d, tile), lambda f: (0, f)),
            pl.BlockSpec((tile, d), lambda f: (f, 0)),
        ],
        out_specs=pl.BlockSpec((rows, d), lambda f: (0, 0)),
        out_shape=jax.ShapeDtypeStruct((rows, d), BF16),
        scratch_shapes=[pltpu.VMEM((rows, d), F32)],
        compiler_params=params(dimension_semantics=("arbitrary",)),
        name="experts",
    )(x, gate_w, up_w, down_w)


def combine_kernel(pick_ref, back_ref, weight_ref, mixed_ref, out_ref):
    tok = mixed_ref.shape[0]
    rows = dot(pick_ref[...], back_ref[...])
    total = mixed_ref[...]
    routed = None
    for k in range(weight_ref.shape[1]):
        term = rows[k * tok : (k + 1) * tok] * weight_ref[:, k : k + 1]
        routed = term if routed is None else routed + term
    out_ref[...] = (total + routed).astype(BF16)


def combine(pick, back, weight, mixed):
    tok, d = mixed.shape
    slots = back.shape[0]
    tile = 512
    return pl.pallas_call(
        combine_kernel,
        grid=(d // tile,),
        in_specs=[
            pl.BlockSpec(pick.shape, lambda j: (0, 0)),
            pl.BlockSpec((slots, tile), lambda j: (0, j)),
            pl.BlockSpec(weight.shape, lambda j: (0, 0)),
            pl.BlockSpec((tok, tile), lambda j: (0, j)),
        ],
        out_specs=pl.BlockSpec((tok, tile), lambda j: (0, j)),
        out_shape=jax.ShapeDtypeStruct((tok, d), BF16),
        compiler_params=params(dimension_semantics=("arbitrary",)),
        name="combine",
    )(pick, back, weight, mixed)


def local(
    queries,
    kv_latent,
    rope_key,
    latent_norm_gain,
    key_up_weight,
    value_up_weight,
    out_proj,
    residual,
    ffn_gain,
    routes,
    route_weights,
    expert_gate,
    expert_up,
    expert_down,
):
    tok = queries.shape[1]
    d = residual.shape[2]
    topk = routes.shape[2]
    sp_size = lax.axis_size("sp")
    dp_size = lax.axis_size("dp")
    experts = sp_size * dp_size
    capacity = max(2, 2 * tok * topk // experts)
    row_table, col_table = turn_tables(sp_size * tok)
    operands = dict(
        latent=kv_latent[0], key=rope_key[0], lgain=latent_norm_gain[None],
        row_table=row_table, col_table=col_table, routes=routes[0].T,
        q=queries[0], kup=key_up_weight, vup=value_up_weight, res=residual[0],
        oproj=out_proj, gain=ffn_gain[None], weights=route_weights[0].T,
        gate=expert_gate[0], up=expert_up[0], down=expert_down[0],
    )
    fused = capacity % 16 == 0
    results = layer(operands, sp_size, dp_size, capacity, fused)
    if fused:
        normed, layer_out = results
        return (normed[None], layer_out[None])
    normed, mixed, outgoing, pick = results
    blocks = outgoing.reshape(experts, capacity, d)
    slot_rows = exchange(blocks, dp_size, 1).reshape(experts * capacity, d)
    expert_out = expert_rows(slot_rows, expert_gate[0], expert_up[0], expert_down[0])
    back = exchange(expert_out.reshape(blocks.shape), dp_size, 2)
    layer_out = combine(pick, back.reshape(experts * capacity, d), route_weights[0], mixed)
    return (normed[None], layer_out[None])


def solution(mesh):
    in_specs = (
        P("dp", "sp", None),
        P("dp", "sp", None),
        P("dp", "sp", None),
        P(),
        P(),
        P(),
        P(),
        P("dp", "sp", None),
        P(),
        P("dp", "sp", None),
        P("dp", "sp", None),
        P(("sp", "dp"), None, None),
        P(("sp", "dp"), None, None),
        P(("sp", "dp"), None, None),
    )
    out_specs = (P("dp", "sp", None), P("dp", "sp", None))
    return jax.shard_map(local, mesh=mesh, in_specs=in_specs, out_specs=out_specs, check_vma=False)
```

```python
import functools
import types

import jax
import jax.numpy as jnp
import numpy as np
from jax import lax
from jax.experimental import pallas as pl
from jax.experimental.pallas import tpu as pltpu
from jax.sharding import PartitionSpec as P

PLAIN = 64
ROT = 32
QK = PLAIN + ROT
VALUE = 64
GRID_W = 64
GROUP = 4

eps_norm = 1e-06
rope_base = 10000.0
clamp_limit = 7.0
glu_alpha = 1.702

F32 = jnp.float32
BF16 = jnp.bfloat16
MESH_ID = pl.DeviceIdType.MESH
VMEM_LIMIT = 60 * 1024 * 1024
LAYER_VMEM = 61 * 1024 * 1024


def params(**kw):
    return pltpu.CompilerParams(**{'vmem_limit_bytes': VMEM_LIMIT, **kw})


PLANE = 4
CHUNK = 512


def turn_tables(length):
    pair = np.arange(ROT) // 2
    quarter = ROT // 4
    frequency = (rope_base ** (-(2.0 * np.arange(quarter)) / (ROT // 2))).astype(np.float32)
    even = np.arange(ROT) % 2 == 0

    def part(places, mine, plain):
        angle = places.astype(np.float32)[:, None] * frequency[pair % quarter][None, :]
        cosine, sine = np.cos(angle.astype(np.float64)), np.sin(angle.astype(np.float64))
        tables = [cosine, np.where(even, -sine, 0.0), np.where(even, 0.0, sine)]
        wide = []
        for table, rest in zip(tables, plain):
            head = np.concatenate(
                [np.full((len(places), PLAIN), rest), np.where(mine, table, 0.0)], axis=1
            )
            wide += [head] * GROUP
        return np.concatenate(wide, axis=1).astype(np.float32)

    rows = part(np.arange(-(-length // GRID_W)), pair < quarter, (0.0, 0.0, 0.0))
    cols = part(np.arange(GRID_W), pair >= quarter, (1.0, 0.0, 0.0))
    return rows, cols


def exchange_kernel(count, dp_size, src, dst, send_sem, recv_sem, own_sem):
    me = lax.axis_index("sp") * dp_size + lax.axis_index("dp")
    barrier = pltpu.get_barrier_semaphore()

    def place(k):
        return lax.rem(me + k, count)

    def device(k):
        other = place(k)
        return (other // dp_size, lax.rem(other, dp_size))

    def greet(k, _):
        pl.semaphore_signal(barrier, inc=1, device_id=device(k), device_id_type=MESH_ID)
        return 0

    lax.fori_loop(1, count, greet, 0)
    own = pltpu.make_async_copy(src.at[me], dst.at[me], own_sem)
    own.start()
    pl.semaphore_wait(barrier, count - 1)

    def copy(k):
        return pltpu.make_async_remote_copy(
            src_ref=src.at[place(k)],
            dst_ref=dst.at[me],
            send_sem=send_sem.at[k],
            recv_sem=recv_sem.at[k],
            device_id=device(k),
            device_id_type=MESH_ID,
        )

    def start(k, _):
        copy(k).start()
        return 0

    def wait(k, _):
        copy(k).wait()
        return 0

    lax.fori_loop(1, count, start, 0)
    lax.fori_loop(1, count, wait, 0)
    own.wait()


def exchange(blocks, dp_size, collective_id):
    count = blocks.shape[0]
    if blocks.shape[1] % 16:
        return lax.all_to_all(blocks, ("sp", "dp"), split_axis=0, concat_axis=0, tiled=True)
    return pl.pallas_call(
        functools.partial(exchange_kernel, count, dp_size),
        out_shape=jax.ShapeDtypeStruct(blocks.shape, blocks.dtype),
        in_specs=[pl.BlockSpec(memory_space=pl.ANY)],
        out_specs=pl.BlockSpec(memory_space=pl.ANY),
        scratch_shapes=[
            pltpu.SemaphoreType.DMA((count,)),
            pltpu.SemaphoreType.DMA((count,)),
            pltpu.SemaphoreType.DMA,
        ],
        compiler_params=params(collective_id=collective_id, has_side_effects=True),
        name="expert_exchange",
    )(blocks)


def dot(a, b, dims=((1,), (0,))):
    return lax.dot_general(a, b, (dims, ((), ())), preferred_element_type=F32)


def lane_fold(x, op):
    parts = [x[:, i : i + 128] for i in range(0, x.shape[1], 128)]
    return functools.reduce(op, parts)


def layer_kernel(names, sizes, *refs):
    r = types.SimpleNamespace(**dict(zip(names, refs)))
    sp_size, dp_size, experts, capacity, fused = sizes
    sp = lax.axis_index("sp")
    dp = lax.axis_index("dp")
    tok, width = r.latent.shape
    d = r.res.shape[1]
    topk = r.routes.shape[0]
    length = sp_size * tok
    line = sp_size // PLANE
    z, p = sp // PLANE, lax.rem(sp, PLANE)
    x_near = z * PLANE + p + 1 - 2 * lax.rem(p, 2)
    y_near = z * PLANE + lax.rem(p + 2, PLANE)
    p_x, p_y = lax.rem(x_near, PLANE), lax.rem(y_near, PLANE)
    half_rot = ROT // 2
    half = tok // 2
    rows = 2 * GROUP * half
    lanes = GROUP * QK
    sets = r.q.shape[1] // lanes
    groups = sets // 2
    tile = min(512, d)
    me = sp * dp_size + dp

    def column(k):
        return lax.rem(z + k, line) * PLANE + p

    barrier = pltpu.get_barrier_semaphore()

    def greet(place, other_dp):
        pl.semaphore_signal(barrier, inc=1, device_id=(place, other_dp), device_id_type=MESH_ID)

    if fused:
        greeted = sp_size * dp_size - 1

        def greet_other(k, _):
            other = lax.rem(me + k, sp_size * dp_size)
            greet(other // dp_size, lax.rem(other, dp_size))
            return 0

        lax.fori_loop(1, greeted + 1, greet_other, 0)
    else:
        greeted = line + 1

        def greet_line(k, _):
            greet(column(k), dp)
            return 0

        lax.fori_loop(1, line, greet_line, 0)
        greet(x_near, dp)
        greet(y_near, dp)

    loaded = [
        "latent", "key", "lgain", "row_table", "col_table", "routes",
        "q", "kup", "vup", "res", "oproj", "gain",
    ]
    if fused:
        loaded += ["weights", "gate", "up", "down"]
    loads = {
        name: pltpu.make_async_copy(getattr(r, name + "_hbm"), getattr(r, name), r.load_sem.at[i])
        for i, name in enumerate(loaded)
    }
    for name in loaded:
        loads[name].start()
    for name in loaded[:6]:
        loads[name].wait()

    grid_rows = tok // GRID_W
    for s in range(grid_rows):
        wide = r.col_table[...] + r.row_table[pl.ds(sp * grid_rows + s, 1), :]
        for i in range(3):
            r.tab[i, s * GRID_W : (s + 1) * GRID_W, :] = wide[:, i * lanes : (i + 1) * lanes]

    def turn(x, wide):
        return (
            x * r.tab[0, :, :wide]
            + pltpu.roll(x, wide - 1, 1) * r.tab[1, :, :wide]
            + pltpu.roll(x, 1, 1) * r.tab[2, :, :wide]
        )

    blocks = r.blocks
    latent_float = r.latent[...].astype(F32)
    square = jnp.mean(latent_float * latent_float, axis=1, keepdims=True)
    latent = latent_float * lax.rsqrt(square + eps_norm) * r.lgain[...]
    blocks[sp, :tok, :] = latent.astype(BF16)
    key = r.key[...].astype(F32)
    key = jnp.concatenate(
        [jnp.zeros((PLAIN, tok), F32), key, jnp.zeros((128 - QK, tok), F32)], axis=0
    ).T
    key_columns = turn(key, 128).T.astype(BF16)
    blocks[sp, tok:, :tok] = key_columns[PLAIN : PLAIN + half_rot]
    blocks[sp, tok:, tok:] = key_columns[PLAIN + half_rot : QK]
    if fused:
        r.line_routes[z] = jnp.concatenate(
            [r.routes[...], jnp.zeros((8 - topk, tok), jnp.int32)], axis=0
        )

    def remote(src, dst, send, recv, place, other_dp):
        return pltpu.make_async_remote_copy(
            src_ref=src,
            dst_ref=dst,
            send_sem=send,
            recv_sem=recv,
            device_id=(place, other_dp),
            device_id_type=MESH_ID,
        )

    def copy(block, other, slot):
        block = blocks.at[block], r.recv_sem.at[block]
        return remote(block[0], block[0], r.send_sem.at[slot], block[1], other, dp)

    def to_line(k):
        return copy(sp, column(k), k)

    def to_x(k):
        return copy(column(k), x_near, line + k)

    def to_y(k):
        return copy(column(k), y_near, 2 * line + k)

    def relay_y(k):
        return copy(k * PLANE + p_x, y_near, 3 * line + k)

    def relay_x(k):
        return copy(k * PLANE + p_y, x_near, 4 * line + k)

    def arrive(block):
        copy(block, sp, 0).wait_recv()

    def routes_to(k, back=False):
        place = lax.rem(z + line - k, line) if back else z
        ref = r.line_routes.at[place]
        return remote(
            ref, ref, r.route_send.at[k], r.route_recv.at[place], column(k), dp
        )

    def fill(block):
        at = pl.ds(pl.multiple_of(block * tok, tok), tok)
        r.lat[at, :] = blocks[block, :tok, :]
        r.kt[:width, at] = blocks[block, :tok, :].T
        r.kt[width : width + half_rot, at] = blocks[block, tok:, :tok]
        r.kt[width + half_rot :, at] = blocks[block, tok:, tok:]

    loads["q"].wait()
    loads["kup"].wait()

    def prepare(j, _):
        x = r.q[:, pl.ds(pl.multiple_of(j * lanes, 128), lanes)].astype(F32)
        turned = turn(x, lanes) * (QK ** (-0.5))
        up = r.kup[:, pl.ds(pl.multiple_of(j * GROUP * PLAIN, 128), GROUP * PLAIN)]
        for i in range(GROUP):
            plain = turned[:, i * QK : i * QK + PLAIN].astype(BF16)
            absorbed = dot(plain, up[:, i * PLAIN : (i + 1) * PLAIN], ((1,), (1,))).astype(BF16)
            rotary = turned[:, i * QK + PLAIN : (i + 1) * QK].astype(BF16)
            at = slice(i * half, (i + 1) * half)
            for h in range(2):
                mine = slice(h * half, (h + 1) * half)
                r.qs[h * sets + j, at, :width] = absorbed[mine]
                r.qs[h * sets + j, at, width:] = rotary[mine]
        return 0

    pl.semaphore_wait(barrier, greeted)
    to_x(0).start()
    to_y(0).start()

    def start_line(k, _):
        to_line(k).start()
        if fused:
            routes_to(k).start()
        return 0

    lax.fori_loop(1, line, start_line, 0)
    early = sets // 4
    lax.fori_loop(0, early, prepare, 0)

    def pass_on(k, _):
        back = line - k
        arrive(column(back))
        to_x(back).start()
        to_y(back).start()
        return 0

    lax.fori_loop(1, line, pass_on, 0)
    lax.fori_loop(early, sets, prepare, 0)

    def fill_column(k, _):
        fill(k * PLANE + p)
        return 0

    lax.fori_loop(0, line, fill_column, 0)

    def relay(k, _):
        other = lax.rem(z + k, line)
        from_x, from_y = other * PLANE + p_x, other * PLANE + p_y
        arrive(from_x)

        @pl.when(lax.rem(other, 2) == 0)
        def _():
            relay_y(other).start()

        arrive(from_y)

        @pl.when(lax.rem(other, 2) == 1)
        def _():
            relay_x(other).start()

        fill(from_x)
        fill(from_y)
        return 0

    lax.fori_loop(0, line, relay, 0)

    def last(k, _):
        block = lax.rem(z + k, line) * PLANE + (PLANE - 1 - p)
        arrive(block)
        fill(block)
        return 0

    lax.fori_loop(0, line, last, 0)
    for name in ("vup", "res", "oproj", "gain"):
        loads[name].wait()

    chunk = min(CHUNK, length)
    buffers = [(r.scores_a, r.top_a), (r.scores_b, r.top_b)]

    def step(weighed, scored, slot):
        if scored is not None:
            mine = r.qs[pl.ds(2 * scored, 2)].reshape(rows, width + ROT)
            new_scores, new_top = buffers[slot]
        if weighed is not None:
            scores, top = buffers[1 - slot]
            highest = jnp.max(top[...], axis=1, keepdims=True)
        best = total = context = None
        for c in range(0, length, chunk):
            at = slice(c, c + chunk)
            if weighed is not None:
                w = jnp.exp(scores[:, at] - highest)
                part = lane_fold(w, jnp.add)
                seen = dot(w.astype(BF16), r.lat[at, :])
                total = part if total is None else total + part
                context = seen if context is None else context + seen
            if scored is not None:
                fresh = dot(mine, r.kt[:, at])
                new_scores[:, at] = fresh
                part = lane_fold(fresh, jnp.maximum)
                best = part if best is None else jnp.maximum(best, part)
        if scored is not None:
            new_top[...] = best
        if weighed is not None:
            context = context / jnp.sum(total, axis=1, keepdims=True)
            r.context[lax.rem(weighed, groups)] = context.astype(BF16)

    def settle(h):
        at = slice(h * half, (h + 1) * half)
        for j in range(groups):
            heads = [
                dot(
                    r.context[j, i * half : (i + 1) * half],
                    r.vup[:, (j * 2 * GROUP + i) * VALUE : (j * 2 * GROUP + i + 1) * VALUE],
                )
                for i in range(2 * GROUP)
            ]
            spread = 2 * GROUP * VALUE
            r.heads[:, j * spread : (j + 1) * spread] = jnp.concatenate(heads, axis=1).astype(BF16)
        square = jnp.zeros((half, 128), F32)
        for n in range(0, d, tile):
            part = r.res[at, n : n + tile].astype(F32) + dot(r.heads[...], r.oproj[:, n : n + tile])
            r.mixed[at, n : n + tile] = part
            square = square + lane_fold(part * part, jnp.add)
        scale = lax.rsqrt(jnp.sum(square, axis=1, keepdims=True) / d + eps_norm)
        normed = (r.mixed[at, :] * scale * r.gain[...]).astype(BF16)
        r.normed[at, :] = normed
        if fused:
            r.tokens[z, at, :] = normed

    def ship(block, h, up):
        ref = r.tokens.at[block, pl.ds(h * half, half), :]
        slot = ((2 if up else 0) + h) * line + block
        return remote(
            ref, ref, r.ship_send.at[slot], r.ship_recv.at[h * line + block],
            sp + PLANE if up else sp - PLANE, dp,
        )

    def ship_both(block, h, act):
        @pl.when((block <= z) & (z + 1 < line))
        def _():
            act(ship(block, h, True))

        @pl.when((block >= z) & (z > 0))
        def _():
            act(ship(block, h, False))

    def start(c):
        c.start()

    def forward(block, h):
        ship(block, h, True).wait_recv()
        ship_both(block, h, start)

    step(None, 0, 0)

    def two(i, _):
        g = 2 * i
        step(g, g + 1, 1)
        step(g + 1, g + 2, 0)

        @pl.when(g + 2 == groups)
        def _():
            settle(0)
            if fused:
                ship_both(z, 0, start)

        return 0

    lax.fori_loop(0, groups - 1, two, 0)
    step(2 * groups - 2, 2 * groups - 1, 1)
    if fused:

        @pl.when(z > 0)
        def _():
            forward(z - 1, 0)

        @pl.when(z + 1 < line)
        def _():
            forward(z + 1, 0)

    step(2 * groups - 1, None, 0)
    settle(1)

    expert_lane = lax.broadcasted_iota(jnp.int32, (tok, experts), 1)
    slot_lane = lax.broadcasted_iota(jnp.int32, (tok, experts * capacity), 1)
    place_a = lax.broadcasted_iota(jnp.int32, (tok, tok), 0)
    place_b = lax.broadcasted_iota(jnp.int32, (tok, tok), 1)

    def columns(part):
        rest = jnp.zeros((tok - topk, tok), F32)
        return jnp.concatenate([part.astype(F32), rest], axis=0).T

    def pick_rows():
        routes = columns(r.routes[...])
        earlier = (place_b < place_a).astype(BF16)
        taken = jnp.zeros((1, experts), F32)
        picks = []
        for k in range(topk):
            expert = routes[:, k : k + 1].astype(jnp.int32)
            named = (expert_lane == expert).astype(F32)
            before = dot(earlier, named.astype(BF16)) + taken
            rank = jnp.sum(before * named, axis=1, keepdims=True)
            slot = expert * capacity + rank.astype(jnp.int32)
            pick = (slot_lane == slot).astype(F32)
            r.pick[k * tok : (k + 1) * tok, :] = pick.astype(BF16)
            picks.append(pick)
            taken = taken + jnp.sum(named, axis=0, keepdims=True)
        return picks

    if fused:
        ship_both(z, 1, start)
        near = PLANE * dp_size
        mine = p * dp_size + dp
        local_row = lax.broadcasted_iota(jnp.int32, (near, tok), 0)
        slot_row = lax.broadcasted_iota(jnp.int32, (near * capacity, tok), 0)

        def wait_routes(k, _):
            routes_to(k, True).wait_recv()
            return 0

        lax.fori_loop(1, line, wait_routes, 0)

        def give(block, other):
            return remote(
                r.stage.at[block, other], r.inbox.at[block, mine],
                r.give_send.at[block * near + other], r.give_recv.at[block * near + mine],
                z * PLANE + other // dp_size, lax.rem(other, dp_size),
            )

        def given(block, other):
            return remote(
                r.stage.at[block, other], r.inbox.at[block, other],
                r.give_send.at[block * near + other], r.give_recv.at[block * near + other],
                z * PLANE + other // dp_size, lax.rem(other, dp_size),
            )

        def dispatch(block):
            later = (place_a < place_b).astype(F32)
            taken = jnp.zeros((near, 1), F32)
            spread = None
            for k in range(topk):
                route = r.line_routes[block, k : k + 1, :] - z * near
                named = (local_row == route).astype(F32)
                before = dot(named, later) + taken
                slot = local_row.astype(F32) * capacity + before + 1.0
                slot = jnp.sum(named * slot, axis=0, keepdims=True).astype(jnp.int32) - 1
                pick = slot_row == slot
                spread = pick if spread is None else spread | pick
                taken = taken + jnp.sum(named, axis=1, keepdims=True)
            spread = spread.astype(F32).astype(BF16)
            for n in range(0, d, tile):
                part = dot(spread, r.tokens[block, :, n : n + tile]).astype(BF16)
                r.stage[block, :, :, n : n + tile] = part.reshape(near, capacity, tile)
            r.inbox[block, mine] = r.stage[block, mine]

            def send(k, _):
                give(block, lax.rem(mine + k, near)).start()
                return 0

            lax.fori_loop(1, near, send, 0)

        def answer(block, other):
            return remote(
                r.stage.at[block, other], r.back.at[me],
                r.back_send.at[block * near + other], r.back_recv.at[me],
                block * PLANE + other // dp_size, lax.rem(other, dp_size),
            )

        def answer_all(block, act):
            def one(other, _):
                @pl.when((block != z) | (other != mine))
                def _():
                    act(answer(block, other))

                return 0

            lax.fori_loop(0, near, one, 0)

        def expert(block):
            def wait(k, _):
                given(block, lax.rem(mine + k, near)).wait_recv()
                return 0

            lax.fori_loop(1, near, wait, 0)
            def given_out(k, _):
                give(block, lax.rem(mine + k, near)).wait_send()
                return 0

            lax.fori_loop(1, near, given_out, 0)
            x = r.inbox[block].reshape(near * capacity, d)
            for n in range(0, r.gate.shape[1], 256):
                at = slice(n, n + 256)
                gate = jnp.minimum(dot(x, r.gate[:, at]), clamp_limit)
                up = jnp.clip(dot(x, r.up[:, at]), -clamp_limit, clamp_limit)
                hidden = gate * jax.nn.sigmoid(glu_alpha * gate) * (up + 1.0)
                r.hidden[:, at] = hidden.astype(BF16)
            for n in range(0, d, tile):
                part = dot(r.hidden[...], r.down[:, n : n + tile]).astype(BF16)
                r.stage[block, :, :, n : n + tile] = part.reshape(near, capacity, tile)

            @pl.when(block == z)
            def _():
                r.back[me] = r.stage[block, mine]

            answer_all(block, start)

        for name in ("weights", "gate", "up", "down"):
            loads[name].wait()

        def at_hop(t, act):
            toward = jnp.where(z < line // 2, 1, -1)
            block = z + toward * jnp.where(lax.rem(t, 2) == 1, (t + 1) // 2, -(t // 2))

            @pl.when((block >= 0) & (block < line))
            def _():
                act(block)

        lag = 2
        hops = 2 * line - 1

        def hop(t, _):
            def bring(block):
                @pl.when(t > 2)
                def _():
                    forward(block, 0)

                @pl.when(t > 0)
                def _():
                    forward(block, 1)

                dispatch(block)

            @pl.when(t < hops)
            def _():
                at_hop(t, bring)

            @pl.when(t >= lag)
            def _():
                at_hop(t - lag, expert)

            return 0

        lax.fori_loop(0, hops + lag, hop, 0)
        pick_rows()
        weights = columns(r.weights[...])

        def combine(block):
            def wait_back(k, _):
                other = block * near + k

                @pl.when(other != me)
                def _():
                    remote(
                        r.stage.at[0, 0], r.back.at[other],
                        r.back_send.at[0], r.back_recv.at[other], sp, dp,
                    ).wait_recv()

                return 0

            lax.fori_loop(0, near, wait_back, 0)
            span = near * capacity
            pick = r.pick[:, pl.ds(pl.multiple_of(block * span, 128), span)]
            for n in range(0, d, tile):
                back = r.back[pl.ds(block * near, near), :, n : n + tile]
                picked = dot(pick, back.reshape(span, tile))
                total = r.mixed[:, n : n + tile]
                for k in range(topk):
                    total = total + picked[k * tok : (k + 1) * tok] * weights[:, k : k + 1]
                r.mixed[:, n : n + tile] = total

        def combine_hop(t, _):
            at_hop(t, combine)
            return 0

        lax.fori_loop(0, hops, combine_hop, 0)
        r.out[...] = r.mixed[...].astype(BF16)

        def finish(block, _):
            def drain(c):
                c.wait_send()

            for h in range(2):
                ship_both(block, h, drain)
            answer_all(block, drain)

            return 0

        lax.fori_loop(0, line, finish, 0)
    else:
        spread = functools.reduce(jnp.add, pick_rows()).T.astype(BF16)
        r.slots[...] = dot(spread, r.normed[...]).astype(BF16)

    def sent(k, _):
        to_x(k).wait_send()
        to_y(k).wait_send()

        @pl.when(k > 0)
        def _():
            to_line(k).wait_send()
            if fused:
                routes_to(k).wait_send()

        @pl.when(lax.rem(k, 2) == 0)
        def _():
            relay_y(k).wait_send()

        @pl.when(lax.rem(k, 2) == 1)
        def _():
            relay_x(k).wait_send()

        return 0

    lax.fori_loop(0, line, sent, 0)


def layer(operands, sp_size, dp_size, capacity, fused):
    tok, d = operands["res"].shape
    width = operands["latent"].shape[1]
    ff = operands["gate"].shape[1]
    topk = operands["routes"].shape[0]
    experts = sp_size * dp_size
    length = sp_size * tok
    line = sp_size // PLANE
    near = PLANE * dp_size
    slots = experts * capacity
    lanes = GROUP * QK
    sets = operands["q"].shape[1] // lanes
    rows = GROUP * tok
    if not fused:
        operands = {k: v for k, v in operands.items() if k not in ("weights", "gate", "up", "down")}
    inputs = list(operands)
    vmem, dma = pltpu.VMEM, pltpu.SemaphoreType.DMA
    scratch = {name: vmem(operands[name].shape, operands[name].dtype) for name in inputs}
    scratch.update(
        blocks=vmem((sp_size, tok + ROT // 2, width), BF16),
        kt=vmem((width + ROT, length), BF16),
        lat=vmem((length, width), BF16),
        tab=vmem((3, tok, lanes), F32),
        qs=vmem((2 * sets, rows // 2, width + ROT), BF16),
        context=vmem((sets // 2, rows, width), BF16),
        heads=vmem((tok // 2, sets * GROUP * VALUE), BF16),
        scores_a=vmem((rows, length), F32),
        scores_b=vmem((rows, length), F32),
        top_a=vmem((rows, 128), F32),
        top_b=vmem((rows, 128), F32),
        load_sem=dma((len(inputs),)),
        send_sem=dma((5 * line,)),
        recv_sem=dma((sp_size,)),
    )
    outputs = {"normed": jax.ShapeDtypeStruct((tok, d), BF16)}
    if fused:
        outputs["out"] = jax.ShapeDtypeStruct((tok, d), BF16)
        scratch.update(
            mixed=vmem((tok, d), F32),
            pick=vmem((topk * tok, slots), BF16),
            line_routes=vmem((line, 8, tok), jnp.int32),
            tokens=vmem((line, tok, d), BF16),
            stage=vmem((line, near, capacity, d), BF16),
            inbox=vmem((line, near, capacity, d), BF16),
            back=vmem((experts, capacity, d), BF16),
            hidden=vmem((near * capacity, ff), BF16),
            route_send=dma((line,)),
            route_recv=dma((line,)),
            ship_send=dma((4 * line,)),
            ship_recv=dma((2 * line,)),
            give_send=dma((line * near,)),
            give_recv=dma((line * near,)),
            back_send=dma((line * near,)),
            back_recv=dma((experts,)),
        )
    else:
        outputs["mixed"] = jax.ShapeDtypeStruct((tok, d), F32)
        outputs["slots"] = jax.ShapeDtypeStruct((slots, d), BF16)
        outputs["pick"] = jax.ShapeDtypeStruct((topk * tok, slots), BF16)
    names = [name + "_hbm" for name in inputs] + list(outputs) + list(scratch)
    return pl.pallas_call(
        functools.partial(layer_kernel, names, (sp_size, dp_size, experts, capacity, fused)),
        in_specs=[pl.BlockSpec(memory_space=pl.ANY)] * len(inputs),
        out_specs=[pl.BlockSpec(memory_space=pltpu.VMEM)] * len(outputs),
        out_shape=[pltpu.VMEM(o.shape, o.dtype) if fused else o for o in outputs.values()],
        scratch_shapes=list(scratch.values()),
        compiler_params=params(
            collective_id=0, has_side_effects=True, vmem_limit_bytes=LAYER_VMEM
        ),
        name="layer",
    )(*operands.values())


def expert_kernel(x_ref, gate_ref, up_ref, down_ref, out_ref, acc):
    step = pl.program_id(0)
    x = x_ref[...]
    gate = jnp.minimum(dot(x, gate_ref[...]), clamp_limit)
    up = jnp.clip(dot(x, up_ref[...]), -clamp_limit, clamp_limit)
    hidden = (gate * jax.nn.sigmoid(glu_alpha * gate) * (up + 1.0)).astype(BF16)
    part = dot(hidden, down_ref[...])

    @pl.when(step == 0)
    def _():
        acc[...] = part

    @pl.when(step > 0)
    def _():
        acc[...] += part

    @pl.when(step == pl.num_programs(0) - 1)
    def _():
        out_ref[...] = acc[...].astype(BF16)


def expert_rows(x, gate_w, up_w, down_w):
    rows, d = x.shape
    ff = gate_w.shape[1]
    tile = 256
    return pl.pallas_call(
        expert_kernel,
        grid=(ff // tile,),
        in_specs=[
            pl.BlockSpec((rows, d), lambda f: (0, 0)),
            pl.BlockSpec((d, tile), lambda f: (0, f)),
            pl.BlockSpec((d, tile), lambda f: (0, f)),
            pl.BlockSpec((tile, d), lambda f: (f, 0)),
        ],
        out_specs=pl.BlockSpec((rows, d), lambda f: (0, 0)),
        out_shape=jax.ShapeDtypeStruct((rows, d), BF16),
        scratch_shapes=[pltpu.VMEM((rows, d), F32)],
        compiler_params=params(dimension_semantics=("arbitrary",)),
        name="experts",
    )(x, gate_w, up_w, down_w)


def combine_kernel(pick_ref, back_ref, weight_ref, mixed_ref, out_ref):
    tok = mixed_ref.shape[0]
    rows = dot(pick_ref[...], back_ref[...])
    total = mixed_ref[...]
    routed = None
    for k in range(weight_ref.shape[1]):
        term = rows[k * tok : (k + 1) * tok] * weight_ref[:, k : k + 1]
        routed = term if routed is None else routed + term
    out_ref[...] = (total + routed).astype(BF16)


def combine(pick, back, weight, mixed):
    tok, d = mixed.shape
    slots = back.shape[0]
    tile = 512
    return pl.pallas_call(
        combine_kernel,
        grid=(d // tile,),
        in_specs=[
            pl.BlockSpec(pick.shape, lambda j: (0, 0)),
            pl.BlockSpec((slots, tile), lambda j: (0, j)),
            pl.BlockSpec(weight.shape, lambda j: (0, 0)),
            pl.BlockSpec((tok, tile), lambda j: (0, j)),
        ],
        out_specs=pl.BlockSpec((tok, tile), lambda j: (0, j)),
        out_shape=jax.ShapeDtypeStruct((tok, d), BF16),
        compiler_params=params(dimension_semantics=("arbitrary",)),
        name="combine",
    )(pick, back, weight, mixed)


def local(
    queries,
    kv_latent,
    rope_key,
    latent_norm_gain,
    key_up_weight,
    value_up_weight,
    out_proj,
    residual,
    ffn_gain,
    routes,
    route_weights,
    expert_gate,
    expert_up,
    expert_down,
):
    tok = queries.shape[1]
    d = residual.shape[2]
    topk = routes.shape[2]
    sp_size = lax.axis_size("sp")
    dp_size = lax.axis_size("dp")
    experts = sp_size * dp_size
    capacity = max(2, 2 * tok * topk // experts)
    row_table, col_table = turn_tables(sp_size * tok)
    operands = dict(
        latent=kv_latent[0], key=rope_key[0].T, lgain=latent_norm_gain[None],
        row_table=row_table, col_table=col_table, routes=routes[0].T,
        q=queries[0], kup=key_up_weight, vup=value_up_weight, res=residual[0],
        oproj=out_proj, gain=ffn_gain[None], weights=route_weights[0].T,
        gate=expert_gate[0], up=expert_up[0], down=expert_down[0],
    )
    fused = capacity % 16 == 0 and PLANE * dp_size * capacity % 128 == 0
    results = layer(operands, sp_size, dp_size, capacity, fused)
    if fused:
        normed, layer_out = results
        return (normed[None], layer_out[None])
    normed, mixed, outgoing, pick = results
    blocks = outgoing.reshape(experts, capacity, d)
    slot_rows = exchange(blocks, dp_size, 1).reshape(experts * capacity, d)
    expert_out = expert_rows(slot_rows, expert_gate[0], expert_up[0], expert_down[0])
    back = exchange(expert_out.reshape(blocks.shape), dp_size, 2)
    layer_out = combine(pick, back.reshape(experts * capacity, d), route_weights[0], mixed)
    return (normed[None], layer_out[None])


def solution(mesh):
    in_specs = (
        P("dp", "sp", None),
        P("dp", "sp", None),
        P("dp", "sp", None),
        P(),
        P(),
        P(),
        P(),
        P("dp", "sp", None),
        P(),
        P("dp", "sp", None),
        P("dp", "sp", None),
        P(("sp", "dp"), None, None),
        P(("sp", "dp"), None, None),
        P(("sp", "dp"), None, None),
    )
    out_specs = (P("dp", "sp", None), P("dp", "sp", None))
    return jax.shard_map(local, mesh=mesh, in_specs=in_specs, out_specs=out_specs, check_vma=False)
```

```python
import functools
import types

import jax
import jax.numpy as jnp
import numpy as np
from jax import lax
from jax.experimental import pallas as pl
from jax.experimental.pallas import tpu as pltpu
from jax.sharding import PartitionSpec as P

PLAIN = 64
ROT = 32
QK = PLAIN + ROT
VALUE = 64
GRID_W = 64
GROUP = 4

eps_norm = 1e-06
rope_base = 10000.0
clamp_limit = 7.0
glu_alpha = 1.702

F32 = jnp.float32
BF16 = jnp.bfloat16
MESH_ID = pl.DeviceIdType.MESH
VMEM_LIMIT = 60 * 1024 * 1024
LAYER_VMEM = 61 * 1024 * 1024


def params(**kw):
    return pltpu.CompilerParams(**{'vmem_limit_bytes': VMEM_LIMIT, **kw})


PLANE = 4
CHUNK = 512


def turn_tables(length):
    pair = np.arange(ROT) // 2
    quarter = ROT // 4
    frequency = (rope_base ** (-(2.0 * np.arange(quarter)) / (ROT // 2))).astype(np.float32)
    even = np.arange(ROT) % 2 == 0

    def part(places, mine, plain):
        angle = places.astype(np.float32)[:, None] * frequency[pair % quarter][None, :]
        cosine, sine = np.cos(angle.astype(np.float64)), np.sin(angle.astype(np.float64))
        tables = [cosine, np.where(even, -sine, 0.0), np.where(even, 0.0, sine)]
        wide = []
        for table, rest in zip(tables, plain):
            head = np.concatenate(
                [np.full((len(places), PLAIN), rest), np.where(mine, table, 0.0)], axis=1
            )
            wide += [head] * GROUP
        return np.concatenate(wide, axis=1).astype(np.float32)

    rows = part(np.arange(-(-length // GRID_W)), pair < quarter, (0.0, 0.0, 0.0))
    cols = part(np.arange(GRID_W), pair >= quarter, (1.0, 0.0, 0.0))
    return rows, cols


def exchange_kernel(count, dp_size, src, dst, send_sem, recv_sem, own_sem):
    me = lax.axis_index("sp") * dp_size + lax.axis_index("dp")
    barrier = pltpu.get_barrier_semaphore()

    def place(k):
        return lax.rem(me + k, count)

    def device(k):
        other = place(k)
        return (other // dp_size, lax.rem(other, dp_size))

    def greet(k, _):
        pl.semaphore_signal(barrier, inc=1, device_id=device(k), device_id_type=MESH_ID)
        return 0

    lax.fori_loop(1, count, greet, 0)
    own = pltpu.make_async_copy(src.at[me], dst.at[me], own_sem)
    own.start()
    pl.semaphore_wait(barrier, count - 1)

    def copy(k):
        return pltpu.make_async_remote_copy(
            src_ref=src.at[place(k)],
            dst_ref=dst.at[me],
            send_sem=send_sem.at[k],
            recv_sem=recv_sem.at[k],
            device_id=device(k),
            device_id_type=MESH_ID,
        )

    def start(k, _):
        copy(k).start()
        return 0

    def wait(k, _):
        copy(k).wait()
        return 0

    lax.fori_loop(1, count, start, 0)
    lax.fori_loop(1, count, wait, 0)
    own.wait()


def exchange(blocks, dp_size, collective_id):
    count = blocks.shape[0]
    if blocks.shape[1] % 16:
        return lax.all_to_all(blocks, ("sp", "dp"), split_axis=0, concat_axis=0, tiled=True)
    return pl.pallas_call(
        functools.partial(exchange_kernel, count, dp_size),
        out_shape=jax.ShapeDtypeStruct(blocks.shape, blocks.dtype),
        in_specs=[pl.BlockSpec(memory_space=pl.ANY)],
        out_specs=pl.BlockSpec(memory_space=pl.ANY),
        scratch_shapes=[
            pltpu.SemaphoreType.DMA((count,)),
            pltpu.SemaphoreType.DMA((count,)),
            pltpu.SemaphoreType.DMA,
        ],
        compiler_params=params(collective_id=collective_id, has_side_effects=True),
        name="expert_exchange",
    )(blocks)


def dot(a, b, dims=((1,), (0,))):
    return lax.dot_general(a, b, (dims, ((), ())), preferred_element_type=F32)


def lane_fold(x, op):
    parts = [x[:, i : i + 128] for i in range(0, x.shape[1], 128)]
    return functools.reduce(op, parts)


def layer_kernel(names, sizes, *refs):
    r = types.SimpleNamespace(**dict(zip(names, refs)))
    sp_size, dp_size, experts, capacity, fused = sizes
    sp = lax.axis_index("sp")
    dp = lax.axis_index("dp")
    tok, width = r.latent.shape
    d = r.res.shape[1]
    topk = r.routes.shape[0]
    length = sp_size * tok
    line = sp_size // PLANE
    z, p = sp // PLANE, lax.rem(sp, PLANE)
    x_near = z * PLANE + p + 1 - 2 * lax.rem(p, 2)
    y_near = z * PLANE + lax.rem(p + 2, PLANE)
    p_x, p_y = lax.rem(x_near, PLANE), lax.rem(y_near, PLANE)
    half_rot = ROT // 2
    half = tok // 2
    rows = 2 * GROUP * half
    lanes = GROUP * QK
    sets = r.q.shape[1] // lanes
    groups = sets // 2
    tile = min(512, d)
    me = sp * dp_size + dp

    def column(k):
        return lax.rem(z + k, line) * PLANE + p

    barrier = pltpu.get_barrier_semaphore()

    def greet(place, other_dp):
        pl.semaphore_signal(barrier, inc=1, device_id=(place, other_dp), device_id_type=MESH_ID)

    if fused:
        greeted = sp_size * dp_size - 1

        def greet_other(k, _):
            other = lax.rem(me + k, sp_size * dp_size)
            greet(other // dp_size, lax.rem(other, dp_size))
            return 0

        lax.fori_loop(1, greeted + 1, greet_other, 0)
    else:
        greeted = line + 1

        def greet_line(k, _):
            greet(column(k), dp)
            return 0

        lax.fori_loop(1, line, greet_line, 0)
        greet(x_near, dp)
        greet(y_near, dp)

    first = ["latent", "key", "lgain", "row_table", "col_table", "routes"]
    if fused:
        first.append("weights")
    loaded = first + ["q", "kup", "vup", "res", "oproj", "gain"]
    if fused:
        loaded += ["gate", "up", "down"]
    loads = {
        name: pltpu.make_async_copy(getattr(r, name + "_hbm"), getattr(r, name), r.load_sem.at[i])
        for i, name in enumerate(loaded)
    }
    for name in loaded:
        loads[name].start()
    for name in first:
        loads[name].wait()

    grid_rows = tok // GRID_W
    for s in range(grid_rows):
        wide = r.col_table[...] + r.row_table[pl.ds(sp * grid_rows + s, 1), :]
        for i in range(3):
            r.tab[i, s * GRID_W : (s + 1) * GRID_W, :] = wide[:, i * lanes : (i + 1) * lanes]

    def turn(x, wide):
        return (
            x * r.tab[0, :, :wide]
            + pltpu.roll(x, wide - 1, 1) * r.tab[1, :, :wide]
            + pltpu.roll(x, 1, 1) * r.tab[2, :, :wide]
        )

    blocks = r.blocks
    latent_float = r.latent[...].astype(F32)
    square = jnp.mean(latent_float * latent_float, axis=1, keepdims=True)
    latent = latent_float * lax.rsqrt(square + eps_norm) * r.lgain[...]
    blocks[sp, :tok, :] = latent.astype(BF16)
    key = r.key[...].astype(F32)
    key = jnp.concatenate(
        [jnp.zeros((PLAIN, tok), F32), key, jnp.zeros((128 - QK, tok), F32)], axis=0
    ).T
    key_columns = turn(key, 128).T.astype(BF16)
    blocks[sp, tok:, :tok] = key_columns[PLAIN : PLAIN + half_rot]
    blocks[sp, tok:, tok:] = key_columns[PLAIN + half_rot : QK]
    if fused:
        r.line_routes[z] = jnp.concatenate(
            [r.routes[...].astype(F32), r.weights[...], jnp.zeros((8 - 2 * topk, tok), F32)],
            axis=0,
        )

    def remote(src, dst, send, recv, place, other_dp):
        return pltpu.make_async_remote_copy(
            src_ref=src,
            dst_ref=dst,
            send_sem=send,
            recv_sem=recv,
            device_id=(place, other_dp),
            device_id_type=MESH_ID,
        )

    def copy(block, other, slot):
        block = blocks.at[block], r.recv_sem.at[block]
        return remote(block[0], block[0], r.send_sem.at[slot], block[1], other, dp)

    def to_line(k):
        return copy(sp, column(k), k)

    def to_x(k):
        return copy(column(k), x_near, line + k)

    def to_y(k):
        return copy(column(k), y_near, 2 * line + k)

    def relay_y(k):
        return copy(k * PLANE + p_x, y_near, 3 * line + k)

    def relay_x(k):
        return copy(k * PLANE + p_y, x_near, 4 * line + k)

    def arrive(block):
        copy(block, sp, 0).wait_recv()

    def routes_to(k, back=False):
        place = lax.rem(z + line - k, line) if back else z
        ref = r.line_routes.at[place]
        return remote(
            ref, ref, r.route_send.at[k], r.route_recv.at[place], column(k), dp
        )

    def fill(block):
        at = pl.ds(pl.multiple_of(block * tok, tok), tok)
        r.lat[at, :] = blocks[block, :tok, :]
        r.kt[:width, at] = blocks[block, :tok, :].T
        r.kt[width : width + half_rot, at] = blocks[block, tok:, :tok]
        r.kt[width + half_rot :, at] = blocks[block, tok:, tok:]

    loads["q"].wait()
    loads["kup"].wait()

    def prepare(j, _):
        x = r.q[:, pl.ds(pl.multiple_of(j * lanes, 128), lanes)].astype(F32)
        turned = turn(x, lanes) * (QK ** (-0.5))
        up = r.kup[:, pl.ds(pl.multiple_of(j * GROUP * PLAIN, 128), GROUP * PLAIN)]
        for i in range(GROUP):
            plain = turned[:, i * QK : i * QK + PLAIN].astype(BF16)
            absorbed = dot(plain, up[:, i * PLAIN : (i + 1) * PLAIN], ((1,), (1,))).astype(BF16)
            rotary = turned[:, i * QK + PLAIN : (i + 1) * QK].astype(BF16)
            at = slice(i * half, (i + 1) * half)
            for h in range(2):
                mine = slice(h * half, (h + 1) * half)
                r.qs[h * sets + j, at, :width] = absorbed[mine]
                r.qs[h * sets + j, at, width:] = rotary[mine]
        return 0

    pl.semaphore_wait(barrier, greeted)
    to_x(0).start()
    to_y(0).start()

    def start_line(k, _):
        to_line(k).start()
        if fused:
            routes_to(k).start()
        return 0

    lax.fori_loop(1, line, start_line, 0)
    early = sets // 4
    lax.fori_loop(0, early, prepare, 0)

    def pass_on(k, _):
        back = line - k
        arrive(column(back))
        to_x(back).start()
        to_y(back).start()
        return 0

    lax.fori_loop(1, line, pass_on, 0)
    lax.fori_loop(early, sets, prepare, 0)

    def fill_column(k, _):
        fill(k * PLANE + p)
        return 0

    lax.fori_loop(0, line, fill_column, 0)

    def relay(k, _):
        other = lax.rem(z + k, line)
        from_x, from_y = other * PLANE + p_x, other * PLANE + p_y
        arrive(from_x)

        @pl.when(lax.rem(other, 2) == 0)
        def _():
            relay_y(other).start()

        arrive(from_y)

        @pl.when(lax.rem(other, 2) == 1)
        def _():
            relay_x(other).start()

        fill(from_x)
        fill(from_y)
        return 0

    lax.fori_loop(0, line, relay, 0)

    def last(k, _):
        block = lax.rem(z + k, line) * PLANE + (PLANE - 1 - p)
        arrive(block)
        fill(block)
        return 0

    lax.fori_loop(0, line, last, 0)
    for name in ("vup", "res", "oproj", "gain"):
        loads[name].wait()

    chunk = min(CHUNK, length)
    buffers = [(r.scores_a, r.top_a), (r.scores_b, r.top_b)]

    def step(weighed, scored, slot):
        if scored is not None:
            mine = r.qs[pl.ds(2 * scored, 2)].reshape(rows, width + ROT)
            new_scores, new_top = buffers[slot]
        if weighed is not None:
            scores, top = buffers[1 - slot]
            highest = jnp.max(top[...], axis=1, keepdims=True)
        best = total = context = None
        for c in range(0, length, chunk):
            at = slice(c, c + chunk)
            if weighed is not None:
                w = jnp.exp(scores[:, at] - highest)
                part = lane_fold(w, jnp.add)
                seen = dot(w.astype(BF16), r.lat[at, :])
                total = part if total is None else total + part
                context = seen if context is None else context + seen
            if scored is not None:
                fresh = dot(mine, r.kt[:, at])
                new_scores[:, at] = fresh
                part = lane_fold(fresh, jnp.maximum)
                best = part if best is None else jnp.maximum(best, part)
        if scored is not None:
            new_top[...] = best
        if weighed is not None:
            context = context / jnp.sum(total, axis=1, keepdims=True)
            r.context[lax.rem(weighed, groups)] = context.astype(BF16)

    def settle(h):
        at = slice(h * half, (h + 1) * half)
        for j in range(groups):
            heads = [
                dot(
                    r.context[j, i * half : (i + 1) * half],
                    r.vup[:, (j * 2 * GROUP + i) * VALUE : (j * 2 * GROUP + i + 1) * VALUE],
                )
                for i in range(2 * GROUP)
            ]
            spread = 2 * GROUP * VALUE
            r.heads[:, j * spread : (j + 1) * spread] = jnp.concatenate(heads, axis=1).astype(BF16)
        square = jnp.zeros((half, 128), F32)
        for n in range(0, d, tile):
            part = r.res[at, n : n + tile].astype(F32) + dot(r.heads[...], r.oproj[:, n : n + tile])
            r.mixed[at, n : n + tile] = part
            square = square + lane_fold(part * part, jnp.add)
        scale = lax.rsqrt(jnp.sum(square, axis=1, keepdims=True) / d + eps_norm)
        normed = (r.mixed[at, :] * scale * r.gain[...]).astype(BF16)
        r.normed[at, :] = normed
        if fused:
            r.tokens[z, at, :] = normed

    def ship(block, h, up):
        ref = r.tokens.at[block, pl.ds(h * half, half), :]
        slot = ((2 if up else 0) + h) * line + block
        return remote(
            ref, ref, r.ship_send.at[slot], r.ship_recv.at[h * line + block],
            sp + PLANE if up else sp - PLANE, dp,
        )

    def ship_both(block, h, act):
        @pl.when((block <= z) & (z + 1 < line))
        def _():
            act(ship(block, h, True))

        @pl.when((block >= z) & (z > 0))
        def _():
            act(ship(block, h, False))

    def start(c):
        c.start()

    def forward(block, h):
        ship(block, h, True).wait_recv()
        ship_both(block, h, start)

    step(None, 0, 0)

    def two(i, _):
        g = 2 * i
        step(g, g + 1, 1)
        step(g + 1, g + 2, 0)

        @pl.when(g + 2 == groups)
        def _():
            settle(0)
            if fused:
                ship_both(z, 0, start)

        return 0

    lax.fori_loop(0, groups - 1, two, 0)
    step(2 * groups - 2, 2 * groups - 1, 1)
    if fused:

        @pl.when(z > 0)
        def _():
            forward(z - 1, 0)

        @pl.when(z + 1 < line)
        def _():
            forward(z + 1, 0)

    step(2 * groups - 1, None, 0)
    settle(1)

    place_a = lax.broadcasted_iota(jnp.int32, (tok, tok), 0)
    place_b = lax.broadcasted_iota(jnp.int32, (tok, tok), 1)

    earlier = (place_b < place_a).astype(BF16)

    def columns(part):
        rest = jnp.zeros((tok - part.shape[0], tok), F32)
        return jnp.concatenate([part.astype(F32), rest], axis=0).T

    def pick_rows(routes, base, count, dest):
        expert_lane = lax.broadcasted_iota(jnp.int32, (tok, count), 1)
        slot_lane = lax.broadcasted_iota(jnp.int32, (tok, count * capacity), 1)
        taken = jnp.zeros((1, count), F32)
        picks = []
        for k in range(topk):
            expert = routes[:, k : k + 1].astype(jnp.int32) - base
            named = (expert_lane == expert).astype(F32)
            before = dot(earlier, named.astype(BF16)) + taken
            rank = jnp.sum(before * named, axis=1, keepdims=True)
            mine = jnp.sum(named, axis=1, keepdims=True) > 0
            slot = jnp.where(mine, expert * capacity + rank.astype(jnp.int32), -1)
            pick = (slot_lane == slot).astype(F32)
            dest[k * tok : (k + 1) * tok, :] = pick.astype(BF16)
            picks.append(pick)
            taken = taken + jnp.sum(named, axis=0, keepdims=True)
        return picks

    if fused:
        ship_both(z, 1, start)
        near = PLANE * dp_size
        mine = p * dp_size + dp
        local_row = lax.broadcasted_iota(jnp.int32, (near, tok), 0)
        slot_row = lax.broadcasted_iota(jnp.int32, (near * capacity, tok), 0)

        def wait_routes(k, _):
            routes_to(k, True).wait_recv()
            return 0

        lax.fori_loop(1, line, wait_routes, 0)

        def give(block, other):
            return remote(
                r.stage.at[block, other], r.inbox.at[block, mine],
                r.give_send.at[block * near + other], r.give_recv.at[block * near + mine],
                z * PLANE + other // dp_size, lax.rem(other, dp_size),
            )

        def given(block, other):
            return remote(
                r.stage.at[block, other], r.inbox.at[block, other],
                r.give_send.at[block * near + other], r.give_recv.at[block * near + other],
                z * PLANE + other // dp_size, lax.rem(other, dp_size),
            )

        def dispatch(block):
            later = (place_a < place_b).astype(F32)
            taken = jnp.zeros((near, 1), F32)
            spread = None
            for k in range(topk):
                route = r.line_routes[block, k : k + 1, :] - (z * near).astype(F32)
                named = (local_row.astype(F32) == route).astype(F32)
                before = dot(named, later) + taken
                slot = local_row.astype(F32) * capacity + before + 1.0
                slot = jnp.sum(named * slot, axis=0, keepdims=True).astype(jnp.int32) - 1
                pick = slot_row == slot
                spread = pick if spread is None else spread | pick
                taken = taken + jnp.sum(named, axis=1, keepdims=True)
            spread = spread.astype(F32).astype(BF16)
            for n in range(0, d, tile):
                part = dot(spread, r.tokens[block, :, n : n + tile]).astype(BF16)
                r.stage[block, :, :, n : n + tile] = part.reshape(near, capacity, tile)
            r.inbox[block, mine] = r.stage[block, mine]

            def send(k, _):
                give(block, lax.rem(mine + k, near)).start()
                return 0

            lax.fori_loop(1, near, send, 0)

        def answer(block, other):
            return remote(
                r.stage.at[block, other], r.back.at[me],
                r.back_send.at[block * near + other], r.back_recv.at[me],
                block * PLANE + other // dp_size, lax.rem(other, dp_size),
            )

        split = line // 2
        low = z < split
        gate_z = jnp.where(low, split - 1, split)
        beyond = jnp.where(low, split, split - 1)
        base = jnp.where(low, 0, split * near)
        joint = split * near

        def answer_gate(block, other):
            return remote(
                r.stage.at[block, other], r.gate_in.at[me - base],
                r.back_send.at[block * near + other], r.gate_recv.at[me - base],
                gate_z * PLANE + other // dp_size, lax.rem(other, dp_size),
            )

        def answer_all(block, act):
            def one(other, _):
                @pl.when((block != beyond) & ((block != z) | (other != mine)))
                def _():
                    act(answer(block, other))

                @pl.when((block == beyond) & ((gate_z != z) | (other != mine)))
                def _():
                    act(answer_gate(block, other))

                return 0

            lax.fori_loop(0, near, one, 0)

        def expert(block):
            def wait(k, _):
                given(block, lax.rem(mine + k, near)).wait_recv()
                return 0

            lax.fori_loop(1, near, wait, 0)
            def given_out(k, _):
                give(block, lax.rem(mine + k, near)).wait_send()
                return 0

            lax.fori_loop(1, near, given_out, 0)
            x = r.inbox[block].reshape(near * capacity, d)
            for n in range(0, r.gate.shape[1], 256):
                at = slice(n, n + 256)
                gate = jnp.minimum(dot(x, r.gate[:, at]), clamp_limit)
                up = jnp.clip(dot(x, r.up[:, at]), -clamp_limit, clamp_limit)
                hidden = gate * jax.nn.sigmoid(glu_alpha * gate) * (up + 1.0)
                r.hidden[:, at] = hidden.astype(BF16)
            for n in range(0, d, tile):
                part = dot(r.hidden[...], r.down[:, n : n + tile]).astype(BF16)
                r.stage[block, :, :, n : n + tile] = part.reshape(near, capacity, tile)

            @pl.when(block == z)
            def _():
                r.back[me] = r.stage[block, mine]

            @pl.when((block == beyond) & (gate_z == z))
            def _():
                r.gate_in[me - base] = r.stage[block, mine]

            @pl.when(((block < split) != low))
            def _():
                answer_all(block, start)

        def joined(start_from):
            return remote(
                r.gate_out, r.joined, r.join_send, r.join_recv,
                start_from * PLANE + p, dp,
            )

        def join():
            theirs = columns(r.line_routes[beyond])
            pick_rows(theirs, base, joint, r.gate_pick)

            def wait_gate(k, _):
                @pl.when(k != me - base)
                def _():
                    remote(
                        r.stage.at[0, 0], r.gate_in.at[k],
                        r.back_send.at[0], r.gate_recv.at[k], sp, dp,
                    ).wait_recv()

                return 0

            lax.fori_loop(0, joint, wait_gate, 0)
            for n in range(0, d, tile):
                rows_in = r.gate_in[:, :, n : n + tile].reshape(joint * capacity, tile)
                picked = dot(r.gate_pick[...], rows_in)
                total = None
                for k in range(topk):
                    term = picked[k * tok : (k + 1) * tok] * theirs[:, topk + k : topk + k + 1]
                    total = term if total is None else total + term
                r.gate_out[:, n : n + tile] = total.astype(BF16)
            joined(beyond).start()

        for name in ("gate", "up", "down"):
            loads[name].wait()

        def at_hop(t, act):
            toward = jnp.where(z < line // 2, 1, -1)
            block = z + toward * jnp.where(lax.rem(t, 2) == 1, (t + 1) // 2, -(t // 2))

            @pl.when((block >= 0) & (block < line))
            def _():
                act(block)

        lag = 2
        hops = 2 * line - 1

        def hop(t, _):
            def bring(block):
                @pl.when(t > 2)
                def _():
                    forward(block, 0)

                @pl.when(t > 0)
                def _():
                    forward(block, 1)

                dispatch(block)

            @pl.when(t < hops)
            def _():
                at_hop(t, bring)

            @pl.when(t >= lag)
            def _():
                at_hop(t - lag, expert)

            return 0

        lax.fori_loop(0, hops + lag, hop, 0)

        def answer_late(block, _):
            @pl.when(jnp.logical_not(((block < split) != low)))
            def _():
                answer_all(block, start)

            return 0

        lax.fori_loop(0, line, answer_late, 0)
        rows_of = columns(r.line_routes[z])
        pick_rows(rows_of, 0, experts, r.pick)
        weights = rows_of[:, topk : 2 * topk]

        @pl.when(z == gate_z)
        def _():
            join()


        def combine(block):
            def wait_back(k, _):
                other = block * near + k

                @pl.when(other != me)
                def _():
                    remote(
                        r.stage.at[0, 0], r.back.at[other],
                        r.back_send.at[0], r.back_recv.at[other], sp, dp,
                    ).wait_recv()

                return 0

            lax.fori_loop(0, near, wait_back, 0)
            span = near * capacity
            pick = r.pick[:, pl.ds(pl.multiple_of(block * span, 128), span)]
            for n in range(0, d, tile):
                back = r.back[pl.ds(block * near, near), :, n : n + tile]
                picked = dot(pick, back.reshape(span, tile))
                total = r.mixed[:, n : n + tile]
                for k in range(topk):
                    total = total + picked[k * tok : (k + 1) * tok] * weights[:, k : k + 1]
                r.mixed[:, n : n + tile] = total

        def combine_hop(t, _):
            def mine_only(block):
                @pl.when((z != gate_z) | ((block < split) == low))
                def _():
                    combine(block)

            at_hop(t, mine_only)
            return 0

        lax.fori_loop(0, hops, combine_hop, 0)

        @pl.when(z == gate_z)
        def _():
            joined(beyond).wait_recv()
            joined(beyond).wait_send()
            r.mixed[...] = r.mixed[...] + r.joined[...].astype(F32)

        r.out[...] = r.mixed[...].astype(BF16)

        def finish(block, _):
            def drain(c):
                c.wait_send()

            for h in range(2):
                ship_both(block, h, drain)
            answer_all(block, drain)

            return 0

        lax.fori_loop(0, line, finish, 0)
    else:
        spread = functools.reduce(
            jnp.add, pick_rows(columns(r.routes[...]), 0, experts, r.pick)
        ).T.astype(BF16)
        r.slots[...] = dot(spread, r.normed[...]).astype(BF16)

    def sent(k, _):
        to_x(k).wait_send()
        to_y(k).wait_send()

        @pl.when(k > 0)
        def _():
            to_line(k).wait_send()
            if fused:
                routes_to(k).wait_send()

        @pl.when(lax.rem(k, 2) == 0)
        def _():
            relay_y(k).wait_send()

        @pl.when(lax.rem(k, 2) == 1)
        def _():
            relay_x(k).wait_send()

        return 0

    lax.fori_loop(0, line, sent, 0)


def layer(operands, sp_size, dp_size, capacity, fused):
    tok, d = operands["res"].shape
    width = operands["latent"].shape[1]
    ff = operands["gate"].shape[1]
    topk = operands["routes"].shape[0]
    experts = sp_size * dp_size
    length = sp_size * tok
    line = sp_size // PLANE
    near = PLANE * dp_size
    slots = experts * capacity
    lanes = GROUP * QK
    sets = operands["q"].shape[1] // lanes
    rows = GROUP * tok
    if not fused:
        operands = {k: v for k, v in operands.items() if k not in ("weights", "gate", "up", "down")}
    inputs = list(operands)
    vmem, dma = pltpu.VMEM, pltpu.SemaphoreType.DMA
    scratch = {name: vmem(operands[name].shape, operands[name].dtype) for name in inputs}
    scratch.update(
        blocks=vmem((sp_size, tok + ROT // 2, width), BF16),
        kt=vmem((width + ROT, length), BF16),
        lat=vmem((length, width), BF16),
        tab=vmem((3, tok, lanes), F32),
        qs=vmem((2 * sets, rows // 2, width + ROT), BF16),
        context=vmem((sets // 2, rows, width), BF16),
        heads=vmem((tok // 2, sets * GROUP * VALUE), BF16),
        scores_a=vmem((rows, length), F32),
        scores_b=vmem((rows, length), F32),
        top_a=vmem((rows, 128), F32),
        top_b=vmem((rows, 128), F32),
        load_sem=dma((len(inputs),)),
        send_sem=dma((5 * line,)),
        recv_sem=dma((sp_size,)),
    )
    outputs = {"normed": jax.ShapeDtypeStruct((tok, d), BF16)}
    if fused:
        outputs["out"] = jax.ShapeDtypeStruct((tok, d), BF16)
        scratch.update(
            mixed=vmem((tok, d), F32),
            pick=vmem((topk * tok, slots), BF16),
            line_routes=vmem((line, 8, tok), F32),
            tokens=vmem((line, tok, d), BF16),
            stage=vmem((line, near, capacity, d), BF16),
            inbox=vmem((line, near, capacity, d), BF16),
            back=vmem((experts, capacity, d), BF16),
            hidden=vmem((near * capacity, ff), BF16),
            route_send=dma((line,)),
            route_recv=dma((line,)),
            ship_send=dma((4 * line,)),
            ship_recv=dma((2 * line,)),
            give_send=dma((line * near,)),
            give_recv=dma((line * near,)),
            back_send=dma((line * near,)),
            back_recv=dma((experts,)),
            gate_in=vmem((line // 2 * near, capacity, d), BF16),
            gate_out=vmem((tok, d), BF16),
            gate_pick=vmem((topk * tok, line // 2 * near * capacity), BF16),
            joined=vmem((tok, d), BF16),
            gate_recv=dma((line // 2 * near,)),
            join_send=dma,
            join_recv=dma,
        )
    else:
        outputs["mixed"] = jax.ShapeDtypeStruct((tok, d), F32)
        outputs["slots"] = jax.ShapeDtypeStruct((slots, d), BF16)
        outputs["pick"] = jax.ShapeDtypeStruct((topk * tok, slots), BF16)
    names = [name + "_hbm" for name in inputs] + list(outputs) + list(scratch)
    return pl.pallas_call(
        functools.partial(layer_kernel, names, (sp_size, dp_size, experts, capacity, fused)),
        in_specs=[pl.BlockSpec(memory_space=pl.ANY)] * len(inputs),
        out_specs=[pl.BlockSpec(memory_space=pltpu.VMEM)] * len(outputs),
        out_shape=[pltpu.VMEM(o.shape, o.dtype) if fused else o for o in outputs.values()],
        scratch_shapes=list(scratch.values()),
        compiler_params=params(
            collective_id=0, has_side_effects=True, vmem_limit_bytes=LAYER_VMEM
        ),
        name="layer",
    )(*operands.values())


def expert_kernel(x_ref, gate_ref, up_ref, down_ref, out_ref, acc):
    step = pl.program_id(0)
    x = x_ref[...]
    gate = jnp.minimum(dot(x, gate_ref[...]), clamp_limit)
    up = jnp.clip(dot(x, up_ref[...]), -clamp_limit, clamp_limit)
    hidden = (gate * jax.nn.sigmoid(glu_alpha * gate) * (up + 1.0)).astype(BF16)
    part = dot(hidden, down_ref[...])

    @pl.when(step == 0)
    def _():
        acc[...] = part

    @pl.when(step > 0)
    def _():
        acc[...] += part

    @pl.when(step == pl.num_programs(0) - 1)
    def _():
        out_ref[...] = acc[...].astype(BF16)


def expert_rows(x, gate_w, up_w, down_w):
    rows, d = x.shape
    ff = gate_w.shape[1]
    tile = 256
    return pl.pallas_call(
        expert_kernel,
        grid=(ff // tile,),
        in_specs=[
            pl.BlockSpec((rows, d), lambda f: (0, 0)),
            pl.BlockSpec((d, tile), lambda f: (0, f)),
            pl.BlockSpec((d, tile), lambda f: (0, f)),
            pl.BlockSpec((tile, d), lambda f: (f, 0)),
        ],
        out_specs=pl.BlockSpec((rows, d), lambda f: (0, 0)),
        out_shape=jax.ShapeDtypeStruct((rows, d), BF16),
        scratch_shapes=[pltpu.VMEM((rows, d), F32)],
        compiler_params=params(dimension_semantics=("arbitrary",)),
        name="experts",
    )(x, gate_w, up_w, down_w)


def combine_kernel(pick_ref, back_ref, weight_ref, mixed_ref, out_ref):
    tok = mixed_ref.shape[0]
    rows = dot(pick_ref[...], back_ref[...])
    total = mixed_ref[...]
    routed = None
    for k in range(weight_ref.shape[1]):
        term = rows[k * tok : (k + 1) * tok] * weight_ref[:, k : k + 1]
        routed = term if routed is None else routed + term
    out_ref[...] = (total + routed).astype(BF16)


def combine(pick, back, weight, mixed):
    tok, d = mixed.shape
    slots = back.shape[0]
    tile = 512
    return pl.pallas_call(
        combine_kernel,
        grid=(d // tile,),
        in_specs=[
            pl.BlockSpec(pick.shape, lambda j: (0, 0)),
            pl.BlockSpec((slots, tile), lambda j: (0, j)),
            pl.BlockSpec(weight.shape, lambda j: (0, 0)),
            pl.BlockSpec((tok, tile), lambda j: (0, j)),
        ],
        out_specs=pl.BlockSpec((tok, tile), lambda j: (0, j)),
        out_shape=jax.ShapeDtypeStruct((tok, d), BF16),
        compiler_params=params(dimension_semantics=("arbitrary",)),
        name="combine",
    )(pick, back, weight, mixed)


def local(
    queries,
    kv_latent,
    rope_key,
    latent_norm_gain,
    key_up_weight,
    value_up_weight,
    out_proj,
    residual,
    ffn_gain,
    routes,
    route_weights,
    expert_gate,
    expert_up,
    expert_down,
):
    tok = queries.shape[1]
    d = residual.shape[2]
    topk = routes.shape[2]
    sp_size = lax.axis_size("sp")
    dp_size = lax.axis_size("dp")
    experts = sp_size * dp_size
    capacity = max(2, 2 * tok * topk // experts)
    row_table, col_table = turn_tables(sp_size * tok)
    operands = dict(
        latent=kv_latent[0], key=rope_key[0].T, lgain=latent_norm_gain[None],
        row_table=row_table, col_table=col_table, routes=routes[0].T,
        q=queries[0], kup=key_up_weight, vup=value_up_weight, res=residual[0],
        oproj=out_proj, gain=ffn_gain[None], weights=route_weights[0].T,
        gate=expert_gate[0], up=expert_up[0], down=expert_down[0],
    )
    fused = capacity % 16 == 0 and PLANE * dp_size * capacity % 128 == 0
    fused = fused and sp_size % (2 * PLANE) == 0
    results = layer(operands, sp_size, dp_size, capacity, fused)
    if fused:
        normed, layer_out = results
        return (normed[None], layer_out[None])
    normed, mixed, outgoing, pick = results
    blocks = outgoing.reshape(experts, capacity, d)
    slot_rows = exchange(blocks, dp_size, 1).reshape(experts * capacity, d)
    expert_out = expert_rows(slot_rows, expert_gate[0], expert_up[0], expert_down[0])
    back = exchange(expert_out.reshape(blocks.shape), dp_size, 2)
    layer_out = combine(pick, back.reshape(experts * capacity, d), route_weights[0], mixed)
    return (normed[None], layer_out[None])


def solution(mesh):
    in_specs = (
        P("dp", "sp", None),
        P("dp", "sp", None),
        P("dp", "sp", None),
        P(),
        P(),
        P(),
        P(),
        P("dp", "sp", None),
        P(),
        P("dp", "sp", None),
        P("dp", "sp", None),
        P(("sp", "dp"), None, None),
        P(("sp", "dp"), None, None),
        P(("sp", "dp"), None, None),
    )
    out_specs = (P("dp", "sp", None), P("dp", "sp", None))
    return jax.shard_map(local, mesh=mesh, in_specs=in_specs, out_specs=out_specs, check_vma=False)
```

```python
import functools
import types

import jax
import jax.numpy as jnp
import numpy as np
from jax import lax
from jax.experimental import pallas as pl
from jax.experimental.pallas import tpu as pltpu
from jax.sharding import PartitionSpec as P

PLAIN = 64
ROT = 32
QK = PLAIN + ROT
VALUE = 64
GRID_W = 64
GROUP = 4

eps_norm = 1e-06
rope_base = 10000.0
clamp_limit = 7.0
glu_alpha = 1.702

F32 = jnp.float32
BF16 = jnp.bfloat16
MESH_ID = pl.DeviceIdType.MESH
VMEM_LIMIT = 60 * 1024 * 1024
LAYER_VMEM = 61 * 1024 * 1024


def params(**kw):
    return pltpu.CompilerParams(**{'vmem_limit_bytes': VMEM_LIMIT, **kw})


PLANE = 4
CHUNK = 512


def turn_tables(length):
    pair = np.arange(ROT) // 2
    quarter = ROT // 4
    frequency = (rope_base ** (-(2.0 * np.arange(quarter)) / (ROT // 2))).astype(np.float32)
    even = np.arange(ROT) % 2 == 0

    def part(places, mine, plain):
        angle = places.astype(np.float32)[:, None] * frequency[pair % quarter][None, :]
        cosine, sine = np.cos(angle.astype(np.float64)), np.sin(angle.astype(np.float64))
        tables = [cosine, np.where(even, -sine, 0.0), np.where(even, 0.0, sine)]
        wide = []
        for table, rest in zip(tables, plain):
            head = np.concatenate(
                [np.full((len(places), PLAIN), rest), np.where(mine, table, 0.0)], axis=1
            )
            wide += [head] * GROUP
        return np.concatenate(wide, axis=1).astype(np.float32)

    rows = part(np.arange(-(-length // GRID_W)), pair < quarter, (0.0, 0.0, 0.0))
    cols = part(np.arange(GRID_W), pair >= quarter, (1.0, 0.0, 0.0))
    return rows, cols


def exchange_kernel(count, dp_size, src, dst, send_sem, recv_sem, own_sem):
    me = lax.axis_index("sp") * dp_size + lax.axis_index("dp")
    barrier = pltpu.get_barrier_semaphore()

    def place(k):
        return lax.rem(me + k, count)

    def device(k):
        other = place(k)
        return (other // dp_size, lax.rem(other, dp_size))

    def greet(k, _):
        pl.semaphore_signal(barrier, inc=1, device_id=device(k), device_id_type=MESH_ID)
        return 0

    lax.fori_loop(1, count, greet, 0)
    own = pltpu.make_async_copy(src.at[me], dst.at[me], own_sem)
    own.start()
    pl.semaphore_wait(barrier, count - 1)

    def copy(k):
        return pltpu.make_async_remote_copy(
            src_ref=src.at[place(k)],
            dst_ref=dst.at[me],
            send_sem=send_sem.at[k],
            recv_sem=recv_sem.at[k],
            device_id=device(k),
            device_id_type=MESH_ID,
        )

    def start(k, _):
        copy(k).start()
        return 0

    def wait(k, _):
        copy(k).wait()
        return 0

    lax.fori_loop(1, count, start, 0)
    lax.fori_loop(1, count, wait, 0)
    own.wait()


def exchange(blocks, dp_size, collective_id):
    count = blocks.shape[0]
    if blocks.shape[1] % 16:
        return lax.all_to_all(blocks, ("sp", "dp"), split_axis=0, concat_axis=0, tiled=True)
    return pl.pallas_call(
        functools.partial(exchange_kernel, count, dp_size),
        out_shape=jax.ShapeDtypeStruct(blocks.shape, blocks.dtype),
        in_specs=[pl.BlockSpec(memory_space=pl.ANY)],
        out_specs=pl.BlockSpec(memory_space=pl.ANY),
        scratch_shapes=[
            pltpu.SemaphoreType.DMA((count,)),
            pltpu.SemaphoreType.DMA((count,)),
            pltpu.SemaphoreType.DMA,
        ],
        compiler_params=params(collective_id=collective_id, has_side_effects=True),
        name="expert_exchange",
    )(blocks)


def dot(a, b, dims=((1,), (0,))):
    return lax.dot_general(a, b, (dims, ((), ())), preferred_element_type=F32)


def lane_fold(x, op):
    parts = [x[:, i : i + 128] for i in range(0, x.shape[1], 128)]
    return functools.reduce(op, parts)


def layer_kernel(names, sizes, *refs):
    r = types.SimpleNamespace(**dict(zip(names, refs)))
    sp_size, dp_size, experts, capacity, fused = sizes
    sp = lax.axis_index("sp")
    dp = lax.axis_index("dp")
    tok, width = r.latent.shape
    d = r.res.shape[1]
    topk = r.routes.shape[0]
    length = sp_size * tok
    line = sp_size // PLANE
    z, p = sp // PLANE, lax.rem(sp, PLANE)
    x_near = z * PLANE + p + 1 - 2 * lax.rem(p, 2)
    y_near = z * PLANE + lax.rem(p + 2, PLANE)
    p_x, p_y = lax.rem(x_near, PLANE), lax.rem(y_near, PLANE)
    half_rot = ROT // 2
    half = tok // 2
    rows = 2 * GROUP * half
    lanes = GROUP * QK
    sets = r.q.shape[1] // lanes
    groups = sets // 2
    tile = min(512, d)
    me = sp * dp_size + dp

    def column(k):
        return lax.rem(z + k, line) * PLANE + p

    barrier = pltpu.get_barrier_semaphore()

    def greet(place, other_dp):
        pl.semaphore_signal(barrier, inc=1, device_id=(place, other_dp), device_id_type=MESH_ID)

    if fused:
        greeted = sp_size * dp_size - 1

        def greet_other(k, _):
            other = lax.rem(me + k, sp_size * dp_size)
            greet(other // dp_size, lax.rem(other, dp_size))
            return 0

        lax.fori_loop(1, greeted + 1, greet_other, 0)
    else:
        greeted = line + 1

        def greet_line(k, _):
            greet(column(k), dp)
            return 0

        lax.fori_loop(1, line, greet_line, 0)
        greet(x_near, dp)
        greet(y_near, dp)

    first = ["latent", "key", "lgain", "row_table", "col_table", "routes"]
    if fused:
        first.append("weights")
    loaded = first + ["q", "kup", "vup", "res", "oproj", "gain"]
    if fused:
        loaded += ["gate", "up", "down"]
    loads = {
        name: pltpu.make_async_copy(getattr(r, name + "_hbm"), getattr(r, name), r.load_sem.at[i])
        for i, name in enumerate(loaded)
    }
    for name in loaded:
        loads[name].start()
    for name in first:
        loads[name].wait()

    grid_rows = tok // GRID_W
    for s in range(grid_rows):
        wide = r.col_table[...] + r.row_table[pl.ds(sp * grid_rows + s, 1), :]
        for i in range(3):
            r.tab[i, s * GRID_W : (s + 1) * GRID_W, :] = wide[:, i * lanes : (i + 1) * lanes]

    def turn(x, wide):
        return (
            x * r.tab[0, :, :wide]
            + pltpu.roll(x, wide - 1, 1) * r.tab[1, :, :wide]
            + pltpu.roll(x, 1, 1) * r.tab[2, :, :wide]
        )

    blocks = r.blocks
    latent_float = r.latent[...].astype(F32)
    square = jnp.mean(latent_float * latent_float, axis=1, keepdims=True)
    latent = latent_float * lax.rsqrt(square + eps_norm) * r.lgain[...]
    blocks[sp, :tok, :] = latent.astype(BF16)
    key = r.key[...].astype(F32)
    key = jnp.concatenate(
        [jnp.zeros((PLAIN, tok), F32), key, jnp.zeros((128 - QK, tok), F32)], axis=0
    ).T
    key_columns = turn(key, 128).T.astype(BF16)
    blocks[sp, tok:, :tok] = key_columns[PLAIN : PLAIN + half_rot]
    blocks[sp, tok:, tok:] = key_columns[PLAIN + half_rot : QK]
    if fused:
        r.line_routes[z] = jnp.concatenate(
            [r.routes[...].astype(F32), r.weights[...], jnp.zeros((8 - 2 * topk, tok), F32)],
            axis=0,
        )

    def remote(src, dst, send, recv, place, other_dp):
        return pltpu.make_async_remote_copy(
            src_ref=src,
            dst_ref=dst,
            send_sem=send,
            recv_sem=recv,
            device_id=(place, other_dp),
            device_id_type=MESH_ID,
        )

    def copy(block, other, slot):
        block = blocks.at[block], r.recv_sem.at[block]
        return remote(block[0], block[0], r.send_sem.at[slot], block[1], other, dp)

    def to_line(k):
        return copy(sp, column(k), k)

    def to_x(k):
        return copy(column(k), x_near, line + k)

    def to_y(k):
        return copy(column(k), y_near, 2 * line + k)

    def relay_y(k):
        return copy(k * PLANE + p_x, y_near, 3 * line + k)

    def relay_x(k):
        return copy(k * PLANE + p_y, x_near, 4 * line + k)

    def arrive(block):
        copy(block, sp, 0).wait_recv()

    def routes_to(k, back=False):
        place = lax.rem(z + line - k, line) if back else z
        ref = r.line_routes.at[place]
        return remote(
            ref, ref, r.route_send.at[k], r.route_recv.at[place], column(k), dp
        )

    def fill(block):
        at = pl.ds(pl.multiple_of(block * tok, tok), tok)
        r.lat[at, :] = blocks[block, :tok, :]
        r.kt[:width, at] = blocks[block, :tok, :].T
        r.kt[width : width + half_rot, at] = blocks[block, tok:, :tok]
        r.kt[width + half_rot :, at] = blocks[block, tok:, tok:]

    loads["q"].wait()
    loads["kup"].wait()

    def prepare(j, _):
        x = r.q[:, pl.ds(pl.multiple_of(j * lanes, 128), lanes)].astype(F32)
        turned = turn(x, lanes) * (QK ** (-0.5))
        up = r.kup[:, pl.ds(pl.multiple_of(j * GROUP * PLAIN, 128), GROUP * PLAIN)]
        for i in range(GROUP):
            plain = turned[:, i * QK : i * QK + PLAIN].astype(BF16)
            absorbed = dot(plain, up[:, i * PLAIN : (i + 1) * PLAIN], ((1,), (1,))).astype(BF16)
            rotary = turned[:, i * QK + PLAIN : (i + 1) * QK].astype(BF16)
            at = slice(i * half, (i + 1) * half)
            for h in range(2):
                mine = slice(h * half, (h + 1) * half)
                r.qs[h * sets + j, at, :width] = absorbed[mine]
                r.qs[h * sets + j, at, width:] = rotary[mine]
        return 0

    pl.semaphore_wait(barrier, greeted)
    to_x(0).start()
    to_y(0).start()

    def start_line(k, _):
        to_line(k).start()
        if fused:
            routes_to(k).start()
        return 0

    lax.fori_loop(1, line, start_line, 0)
    early = sets // 4
    lax.fori_loop(0, early, prepare, 0)

    def pass_on(k, _):
        back = line - k
        arrive(column(back))
        to_x(back).start()
        to_y(back).start()
        return 0

    lax.fori_loop(1, line, pass_on, 0)
    lax.fori_loop(early, sets, prepare, 0)

    def fill_column(k, _):
        fill(k * PLANE + p)
        return 0

    lax.fori_loop(0, line, fill_column, 0)

    def relay(k, _):
        other = lax.rem(z + k, line)
        from_x, from_y = other * PLANE + p_x, other * PLANE + p_y
        arrive(from_x)

        @pl.when(lax.rem(other, 2) == 0)
        def _():
            relay_y(other).start()

        arrive(from_y)

        @pl.when(lax.rem(other, 2) == 1)
        def _():
            relay_x(other).start()

        fill(from_x)
        fill(from_y)
        return 0

    lax.fori_loop(0, line, relay, 0)

    def last(k, _):
        block = lax.rem(z + k, line) * PLANE + (PLANE - 1 - p)
        arrive(block)
        fill(block)
        return 0

    lax.fori_loop(0, line, last, 0)
    for name in ("vup", "res", "oproj", "gain"):
        loads[name].wait()

    chunk = min(CHUNK, length)
    buffers = [(r.scores_a, r.top_a), (r.scores_b, r.top_b)]

    def step(weighed, scored, slot):
        if scored is not None:
            mine = r.qs[pl.ds(2 * scored, 2)].reshape(rows, width + ROT)
            new_scores, new_top = buffers[slot]
        if weighed is not None:
            scores, top = buffers[1 - slot]
            highest = jnp.max(top[...], axis=1, keepdims=True)
        best = total = context = None
        for c in range(0, length, chunk):
            at = slice(c, c + chunk)
            if weighed is not None:
                w = jnp.exp(scores[:, at] - highest)
                part = lane_fold(w, jnp.add)
                seen = dot(w.astype(BF16), r.lat[at, :])
                total = part if total is None else total + part
                context = seen if context is None else context + seen
            if scored is not None:
                fresh = dot(mine, r.kt[:, at])
                new_scores[:, at] = fresh
                part = lane_fold(fresh, jnp.maximum)
                best = part if best is None else jnp.maximum(best, part)
        if scored is not None:
            new_top[...] = best
        if weighed is not None:
            context = context / jnp.sum(total, axis=1, keepdims=True)
            r.context[lax.rem(weighed, groups)] = context.astype(BF16)

    def settle(h):
        at = slice(h * half, (h + 1) * half)
        for j in range(groups):
            heads = [
                dot(
                    r.context[j, i * half : (i + 1) * half],
                    r.vup[:, (j * 2 * GROUP + i) * VALUE : (j * 2 * GROUP + i + 1) * VALUE],
                )
                for i in range(2 * GROUP)
            ]
            spread = 2 * GROUP * VALUE
            r.heads[:, j * spread : (j + 1) * spread] = jnp.concatenate(heads, axis=1).astype(BF16)
        square = jnp.zeros((half, 128), F32)
        for n in range(0, d, tile):
            part = r.res[at, n : n + tile].astype(F32) + dot(r.heads[...], r.oproj[:, n : n + tile])
            r.mixed[at, n : n + tile] = part
            square = square + lane_fold(part * part, jnp.add)
        scale = lax.rsqrt(jnp.sum(square, axis=1, keepdims=True) / d + eps_norm)
        normed = (r.mixed[at, :] * scale * r.gain[...]).astype(BF16)
        r.normed[at, :] = normed
        if fused:
            r.tokens[z, at, :] = normed

    def ship(block, h, up):
        ref = r.tokens.at[block, pl.ds(h * half, half), :]
        slot = ((2 if up else 0) + h) * line + block
        return remote(
            ref, ref, r.ship_send.at[slot], r.ship_recv.at[h * line + block],
            sp + PLANE if up else sp - PLANE, dp,
        )

    def ship_both(block, h, act):
        @pl.when((block <= z) & (z + 1 < line))
        def _():
            act(ship(block, h, True))

        @pl.when((block >= z) & (z > 0))
        def _():
            act(ship(block, h, False))

    def start(c):
        c.start()

    def forward(block, h):
        ship(block, h, True).wait_recv()
        ship_both(block, h, start)

    step(None, 0, 0)

    def two(i, _):
        g = 2 * i
        step(g, g + 1, 1)
        step(g + 1, g + 2, 0)

        @pl.when(g + 2 == groups)
        def _():
            settle(0)
            if fused:
                ship_both(z, 0, start)

        return 0

    lax.fori_loop(0, groups - 1, two, 0)
    step(2 * groups - 2, 2 * groups - 1, 1)
    if fused:

        @pl.when(z > 0)
        def _():
            forward(z - 1, 0)

        @pl.when(z + 1 < line)
        def _():
            forward(z + 1, 0)

    step(2 * groups - 1, None, 0)
    settle(1)

    place_a = lax.broadcasted_iota(jnp.int32, (tok, tok), 0)
    place_b = lax.broadcasted_iota(jnp.int32, (tok, tok), 1)

    earlier = (place_b < place_a).astype(BF16)

    def columns(part):
        rest = jnp.zeros((tok - part.shape[0], tok), F32)
        return jnp.concatenate([part.astype(F32), rest], axis=0).T

    def pick_rows(routes, base, count, dest):
        expert_lane = lax.broadcasted_iota(jnp.int32, (tok, count), 1)
        slot_lane = lax.broadcasted_iota(jnp.int32, (tok, count * capacity), 1)
        taken = jnp.zeros((1, count), F32)
        picks = []
        for k in range(topk):
            expert = routes[:, k : k + 1].astype(jnp.int32) - base
            named = (expert_lane == expert).astype(F32)
            before = dot(earlier, named.astype(BF16)) + taken
            rank = jnp.sum(before * named, axis=1, keepdims=True)
            mine = jnp.sum(named, axis=1, keepdims=True) > 0
            slot = jnp.where(mine, expert * capacity + rank.astype(jnp.int32), -1)
            pick = (slot_lane == slot).astype(F32)
            dest[k * tok : (k + 1) * tok, :] = pick.astype(BF16)
            picks.append(pick)
            taken = taken + jnp.sum(named, axis=0, keepdims=True)
        return picks

    if fused:
        ship_both(z, 1, start)
        near = PLANE * dp_size
        mine = p * dp_size + dp
        local_row = lax.broadcasted_iota(jnp.int32, (near, tok), 0)
        slot_row = lax.broadcasted_iota(jnp.int32, (near * capacity, tok), 0)

        def wait_routes(k, _):
            routes_to(k, True).wait_recv()
            return 0

        lax.fori_loop(1, line, wait_routes, 0)

        def give(block, other):
            return remote(
                r.stage.at[block, other], r.inbox.at[block, mine],
                r.give_send.at[block * near + other], r.give_recv.at[block * near + mine],
                z * PLANE + other // dp_size, lax.rem(other, dp_size),
            )

        def given(block, other):
            return remote(
                r.stage.at[block, other], r.inbox.at[block, other],
                r.give_send.at[block * near + other], r.give_recv.at[block * near + other],
                z * PLANE + other // dp_size, lax.rem(other, dp_size),
            )

        def dispatch(block):
            later = (place_a < place_b).astype(F32)
            taken = jnp.zeros((near, 1), F32)
            spread = None
            for k in range(topk):
                route = r.line_routes[block, k : k + 1, :] - (z * near).astype(F32)
                named = (local_row.astype(F32) == route).astype(F32)
                before = dot(named, later) + taken
                slot = local_row.astype(F32) * capacity + before + 1.0
                slot = jnp.sum(named * slot, axis=0, keepdims=True).astype(jnp.int32) - 1
                pick = slot_row == slot
                spread = pick if spread is None else spread | pick
                taken = taken + jnp.sum(named, axis=1, keepdims=True)
            spread = spread.astype(F32).astype(BF16)
            for n in range(0, d, tile):
                part = dot(spread, r.tokens[block, :, n : n + tile]).astype(BF16)
                r.stage[block, :, :, n : n + tile] = part.reshape(near, capacity, tile)
            r.inbox[block, mine] = r.stage[block, mine]

            def send(k, _):
                give(block, lax.rem(mine + k, near)).start()
                return 0

            lax.fori_loop(1, near, send, 0)

        def answer(block, other):
            return remote(
                r.stage.at[block, other], r.back.at[me],
                r.back_send.at[block * near + other], r.back_recv.at[me],
                block * PLANE + other // dp_size, lax.rem(other, dp_size),
            )

        split = line // 2
        low = z < split
        gate_z = jnp.where(low, split - 1, split)
        beyond = jnp.where(low, split, split - 1)
        base = jnp.where(low, 0, split * near)
        joint = split * near

        def answer_gate(block, other):
            return remote(
                r.stage.at[block, other], r.gate_in.at[me - base],
                r.back_send.at[block * near + other], r.gate_recv.at[me - base],
                gate_z * PLANE + other // dp_size, lax.rem(other, dp_size),
            )

        def answer_all(block, act):
            def one(k, _):
                other = lax.rem(mine + k, near)

                @pl.when((block != beyond) & ((block != z) | (other != mine)))
                def _():
                    act(answer(block, other))

                @pl.when((block == beyond) & ((gate_z != z) | (other != mine)))
                def _():
                    act(answer_gate(block, other))

                return 0

            lax.fori_loop(0, near, one, 0)

        def expert(block):
            def wait(k, _):
                given(block, lax.rem(mine + k, near)).wait_recv()
                return 0

            lax.fori_loop(1, near, wait, 0)
            def given_out(k, _):
                give(block, lax.rem(mine + k, near)).wait_send()
                return 0

            lax.fori_loop(1, near, given_out, 0)
            x = r.inbox[block].reshape(near * capacity, d)
            for n in range(0, r.gate.shape[1], 256):
                at = slice(n, n + 256)
                gate = jnp.minimum(dot(x, r.gate[:, at]), clamp_limit)
                up = jnp.clip(dot(x, r.up[:, at]), -clamp_limit, clamp_limit)
                hidden = gate * jax.nn.sigmoid(glu_alpha * gate) * (up + 1.0)
                r.hidden[:, at] = hidden.astype(BF16)
            for n in range(0, d, tile):
                part = dot(r.hidden[...], r.down[:, n : n + tile]).astype(BF16)
                r.stage[block, :, :, n : n + tile] = part.reshape(near, capacity, tile)

            @pl.when(block == z)
            def _():
                r.back[me] = r.stage[block, mine]

            @pl.when((block == beyond) & (gate_z == z))
            def _():
                r.gate_in[me - base] = r.stage[block, mine]

            @pl.when(((block < split) != low))
            def _():
                answer_all(block, start)

        def joined(start_from):
            return remote(
                r.gate_out, r.joined, r.join_send, r.join_recv,
                start_from * PLANE + p, dp,
            )

        def join():
            theirs = columns(r.line_routes[beyond])
            pick_rows(theirs, base, joint, r.gate_pick)

            def wait_gate(k, _):
                @pl.when(k != me - base)
                def _():
                    remote(
                        r.stage.at[0, 0], r.gate_in.at[k],
                        r.back_send.at[0], r.gate_recv.at[k], sp, dp,
                    ).wait_recv()

                return 0

            lax.fori_loop(0, joint, wait_gate, 0)
            for n in range(0, d, tile):
                rows_in = r.gate_in[:, :, n : n + tile].reshape(joint * capacity, tile)
                picked = dot(r.gate_pick[...], rows_in)
                total = None
                for k in range(topk):
                    term = picked[k * tok : (k + 1) * tok] * theirs[:, topk + k : topk + k + 1]
                    total = term if total is None else total + term
                r.gate_out[:, n : n + tile] = total.astype(BF16)
            joined(beyond).start()

        for name in ("gate", "up", "down"):
            loads[name].wait()

        def at_hop(t, act):
            toward = jnp.where(z < line // 2, 1, -1)
            block = z + toward * jnp.where(lax.rem(t, 2) == 1, (t + 1) // 2, -(t // 2))

            @pl.when((block >= 0) & (block < line))
            def _():
                act(block)

        lag = 2
        hops = 2 * line - 1

        def hop(t, _):
            def bring(block):
                @pl.when(t > 2)
                def _():
                    forward(block, 0)

                forward(block, 1)

            @pl.when((t < hops) & (lax.rem(t, 2) == 1))
            def _():
                at_hop(t + 1, bring)
                at_hop(t, bring)

            @pl.when(t < hops)
            def _():
                at_hop(t, dispatch)

            @pl.when(t >= lag)
            def _():
                at_hop(t - lag, expert)

            return 0

        lax.fori_loop(0, hops + lag, hop, 0)

        def answer_late(block, _):
            @pl.when(jnp.logical_not(((block < split) != low)))
            def _():
                answer_all(block, start)

            return 0

        lax.fori_loop(0, line, answer_late, 0)
        rows_of = columns(r.line_routes[z])
        pick_rows(rows_of, 0, experts, r.pick)
        weights = rows_of[:, topk : 2 * topk]

        @pl.when(z == gate_z)
        def _():
            join()


        def combine(block):
            def wait_back(k, _):
                other = block * near + k

                @pl.when(other != me)
                def _():
                    remote(
                        r.stage.at[0, 0], r.back.at[other],
                        r.back_send.at[0], r.back_recv.at[other], sp, dp,
                    ).wait_recv()

                return 0

            lax.fori_loop(0, near, wait_back, 0)
            span = near * capacity
            pick = r.pick[:, pl.ds(pl.multiple_of(block * span, 128), span)]
            for n in range(0, d, tile):
                back = r.back[pl.ds(block * near, near), :, n : n + tile]
                picked = dot(pick, back.reshape(span, tile))
                total = r.mixed[:, n : n + tile]
                for k in range(topk):
                    total = total + picked[k * tok : (k + 1) * tok] * weights[:, k : k + 1]
                r.mixed[:, n : n + tile] = total

        def combine_hop(t, _):
            def mine_only(block):
                @pl.when((z != gate_z) | ((block < split) == low))
                def _():
                    combine(block)

            at_hop(t, mine_only)
            return 0

        lax.fori_loop(0, hops, combine_hop, 0)

        @pl.when(z == gate_z)
        def _():
            joined(beyond).wait_recv()
            joined(beyond).wait_send()
            r.mixed[...] = r.mixed[...] + r.joined[...].astype(F32)

        r.out[...] = r.mixed[...].astype(BF16)

        def finish(block, _):
            def drain(c):
                c.wait_send()

            for h in range(2):
                ship_both(block, h, drain)
            answer_all(block, drain)

            return 0

        lax.fori_loop(0, line, finish, 0)
    else:
        spread = functools.reduce(
            jnp.add, pick_rows(columns(r.routes[...]), 0, experts, r.pick)
        ).T.astype(BF16)
        r.slots[...] = dot(spread, r.normed[...]).astype(BF16)

    def sent(k, _):
        to_x(k).wait_send()
        to_y(k).wait_send()

        @pl.when(k > 0)
        def _():
            to_line(k).wait_send()
            if fused:
                routes_to(k).wait_send()

        @pl.when(lax.rem(k, 2) == 0)
        def _():
            relay_y(k).wait_send()

        @pl.when(lax.rem(k, 2) == 1)
        def _():
            relay_x(k).wait_send()

        return 0

    lax.fori_loop(0, line, sent, 0)


def layer(operands, sp_size, dp_size, capacity, fused):
    tok, d = operands["res"].shape
    width = operands["latent"].shape[1]
    ff = operands["gate"].shape[1]
    topk = operands["routes"].shape[0]
    experts = sp_size * dp_size
    length = sp_size * tok
    line = sp_size // PLANE
    near = PLANE * dp_size
    slots = experts * capacity
    lanes = GROUP * QK
    sets = operands["q"].shape[1] // lanes
    rows = GROUP * tok
    if not fused:
        operands = {k: v for k, v in operands.items() if k not in ("weights", "gate", "up", "down")}
    inputs = list(operands)
    vmem, dma = pltpu.VMEM, pltpu.SemaphoreType.DMA
    scratch = {name: vmem(operands[name].shape, operands[name].dtype) for name in inputs}
    scratch.update(
        blocks=vmem((sp_size, tok + ROT // 2, width), BF16),
        kt=vmem((width + ROT, length), BF16),
        lat=vmem((length, width), BF16),
        tab=vmem((3, tok, lanes), F32),
        qs=vmem((2 * sets, rows // 2, width + ROT), BF16),
        context=vmem((sets // 2, rows, width), BF16),
        heads=vmem((tok // 2, sets * GROUP * VALUE), BF16),
        scores_a=vmem((rows, length), F32),
        scores_b=vmem((rows, length), F32),
        top_a=vmem((rows, 128), F32),
        top_b=vmem((rows, 128), F32),
        load_sem=dma((len(inputs),)),
        send_sem=dma((5 * line,)),
        recv_sem=dma((sp_size,)),
    )
    outputs = {"normed": jax.ShapeDtypeStruct((tok, d), BF16)}
    if fused:
        outputs["out"] = jax.ShapeDtypeStruct((tok, d), BF16)
        scratch.update(
            mixed=vmem((tok, d), F32),
            pick=vmem((topk * tok, slots), BF16),
            line_routes=vmem((line, 8, tok), F32),
            tokens=vmem((line, tok, d), BF16),
            stage=vmem((line, near, capacity, d), BF16),
            inbox=vmem((line, near, capacity, d), BF16),
            back=vmem((experts, capacity, d), BF16),
            hidden=vmem((near * capacity, ff), BF16),
            route_send=dma((line,)),
            route_recv=dma((line,)),
            ship_send=dma((4 * line,)),
            ship_recv=dma((2 * line,)),
            give_send=dma((line * near,)),
            give_recv=dma((line * near,)),
            back_send=dma((line * near,)),
            back_recv=dma((experts,)),
            gate_in=vmem((line // 2 * near, capacity, d), BF16),
            gate_out=vmem((tok, d), BF16),
            gate_pick=vmem((topk * tok, line // 2 * near * capacity), BF16),
            joined=vmem((tok, d), BF16),
            gate_recv=dma((line // 2 * near,)),
            join_send=dma,
            join_recv=dma,
        )
    else:
        outputs["mixed"] = jax.ShapeDtypeStruct((tok, d), F32)
        outputs["slots"] = jax.ShapeDtypeStruct((slots, d), BF16)
        outputs["pick"] = jax.ShapeDtypeStruct((topk * tok, slots), BF16)
    names = [name + "_hbm" for name in inputs] + list(outputs) + list(scratch)
    return pl.pallas_call(
        functools.partial(layer_kernel, names, (sp_size, dp_size, experts, capacity, fused)),
        in_specs=[pl.BlockSpec(memory_space=pl.ANY)] * len(inputs),
        out_specs=[pl.BlockSpec(memory_space=pltpu.VMEM)] * len(outputs),
        out_shape=[pltpu.VMEM(o.shape, o.dtype) if fused else o for o in outputs.values()],
        scratch_shapes=list(scratch.values()),
        compiler_params=params(
            collective_id=0, has_side_effects=True, vmem_limit_bytes=LAYER_VMEM
        ),
        name="layer",
    )(*operands.values())


def expert_kernel(x_ref, gate_ref, up_ref, down_ref, out_ref, acc):
    step = pl.program_id(0)
    x = x_ref[...]
    gate = jnp.minimum(dot(x, gate_ref[...]), clamp_limit)
    up = jnp.clip(dot(x, up_ref[...]), -clamp_limit, clamp_limit)
    hidden = (gate * jax.nn.sigmoid(glu_alpha * gate) * (up + 1.0)).astype(BF16)
    part = dot(hidden, down_ref[...])

    @pl.when(step == 0)
    def _():
        acc[...] = part

    @pl.when(step > 0)
    def _():
        acc[...] += part

    @pl.when(step == pl.num_programs(0) - 1)
    def _():
        out_ref[...] = acc[...].astype(BF16)


def expert_rows(x, gate_w, up_w, down_w):
    rows, d = x.shape
    ff = gate_w.shape[1]
    tile = 256
    return pl.pallas_call(
        expert_kernel,
        grid=(ff // tile,),
        in_specs=[
            pl.BlockSpec((rows, d), lambda f: (0, 0)),
            pl.BlockSpec((d, tile), lambda f: (0, f)),
            pl.BlockSpec((d, tile), lambda f: (0, f)),
            pl.BlockSpec((tile, d), lambda f: (f, 0)),
        ],
        out_specs=pl.BlockSpec((rows, d), lambda f: (0, 0)),
        out_shape=jax.ShapeDtypeStruct((rows, d), BF16),
        scratch_shapes=[pltpu.VMEM((rows, d), F32)],
        compiler_params=params(dimension_semantics=("arbitrary",)),
        name="experts",
    )(x, gate_w, up_w, down_w)


def combine_kernel(pick_ref, back_ref, weight_ref, mixed_ref, out_ref):
    tok = mixed_ref.shape[0]
    rows = dot(pick_ref[...], back_ref[...])
    total = mixed_ref[...]
    routed = None
    for k in range(weight_ref.shape[1]):
        term = rows[k * tok : (k + 1) * tok] * weight_ref[:, k : k + 1]
        routed = term if routed is None else routed + term
    out_ref[...] = (total + routed).astype(BF16)


def combine(pick, back, weight, mixed):
    tok, d = mixed.shape
    slots = back.shape[0]
    tile = 512
    return pl.pallas_call(
        combine_kernel,
        grid=(d // tile,),
        in_specs=[
            pl.BlockSpec(pick.shape, lambda j: (0, 0)),
            pl.BlockSpec((slots, tile), lambda j: (0, j)),
            pl.BlockSpec(weight.shape, lambda j: (0, 0)),
            pl.BlockSpec((tok, tile), lambda j: (0, j)),
        ],
        out_specs=pl.BlockSpec((tok, tile), lambda j: (0, j)),
        out_shape=jax.ShapeDtypeStruct((tok, d), BF16),
        compiler_params=params(dimension_semantics=("arbitrary",)),
        name="combine",
    )(pick, back, weight, mixed)


def local(
    queries,
    kv_latent,
    rope_key,
    latent_norm_gain,
    key_up_weight,
    value_up_weight,
    out_proj,
    residual,
    ffn_gain,
    routes,
    route_weights,
    expert_gate,
    expert_up,
    expert_down,
):
    tok = queries.shape[1]
    d = residual.shape[2]
    topk = routes.shape[2]
    sp_size = lax.axis_size("sp")
    dp_size = lax.axis_size("dp")
    experts = sp_size * dp_size
    capacity = max(2, 2 * tok * topk // experts)
    row_table, col_table = turn_tables(sp_size * tok)
    operands = dict(
        latent=kv_latent[0], key=rope_key[0].T, lgain=latent_norm_gain[None],
        row_table=row_table, col_table=col_table, routes=routes[0].T,
        q=queries[0], kup=key_up_weight, vup=value_up_weight, res=residual[0],
        oproj=out_proj, gain=ffn_gain[None], weights=route_weights[0].T,
        gate=expert_gate[0], up=expert_up[0], down=expert_down[0],
    )
    fused = capacity % 16 == 0 and PLANE * dp_size * capacity % 128 == 0
    fused = fused and sp_size % (2 * PLANE) == 0
    results = layer(operands, sp_size, dp_size, capacity, fused)
    if fused:
        normed, layer_out = results
        return (normed[None], layer_out[None])
    normed, mixed, outgoing, pick = results
    blocks = outgoing.reshape(experts, capacity, d)
    slot_rows = exchange(blocks, dp_size, 1).reshape(experts * capacity, d)
    expert_out = expert_rows(slot_rows, expert_gate[0], expert_up[0], expert_down[0])
    back = exchange(expert_out.reshape(blocks.shape), dp_size, 2)
    layer_out = combine(pick, back.reshape(experts * capacity, d), route_weights[0], mixed)
    return (normed[None], layer_out[None])


def solution(mesh):
    in_specs = (
        P("dp", "sp", None),
        P("dp", "sp", None),
        P("dp", "sp", None),
        P(),
        P(),
        P(),
        P(),
        P("dp", "sp", None),
        P(),
        P("dp", "sp", None),
        P("dp", "sp", None),
        P(("sp", "dp"), None, None),
        P(("sp", "dp"), None, None),
        P(("sp", "dp"), None, None),
    )
    out_specs = (P("dp", "sp", None), P("dp", "sp", None))
    return jax.shard_map(local, mesh=mesh, in_specs=in_specs, out_specs=out_specs, check_vma=False)
```
